32 devices in a mesh: ep: 4 (over y, x), tp: 8 (over z, core).
Axes of the slice: x: 2, y: 2, z: 4, core: 2. Of those that a mesh axis runs over, the one named last changes fastest.
Arguments:
- tokens: bfloat16 [64, 4096], P('ep'), may hold values from -6 to 6
- query_weight: bfloat16 [4096, 4096], P('ep', 'tp'), may hold values from -0.09375 to 0.09375
- key_weight: bfloat16 [4096, 2048], P('ep', 'tp'), may hold values from -0.15625 to 0.15625
- value_weight: bfloat16 [4096, 2048], P('ep', 'tp'), may hold values from -0.09375 to 0.09375
- out_weight: bfloat16 [4096, 4096], P('tp', 'ep'), may hold values from -0.09375 to 0.09375
- head_lambda: float32 [32], P('tp'), may hold values from 0.3 to 0.8
- head_gain: float32 [128], replicated, may hold values from 0.1 to 1.9
- key_cache: bfloat16 [64, 1024, 16, 128], P('ep', None, 'tp'), may hold values from -1000 to 1000
- value_cache: bfloat16 [64, 1024, 16, 128], P('ep', None, 'tp'), may hold values from -6 to 6
- lengths: int32 [64], P('ep'), may hold values from 128 to 1024, as said below
- first_gain: float32 [4096], replicated, may hold values from 0.3 to 3
- second_gain: float32 [4096], P('tp'), may hold values from 0.1 to 1.9
- expert_ids: int32 [64, 2], P('ep'), may hold values from 0 to 15, all different within a row; in each aligned block of 16 rows (0 to 15, 16 to 31, ...) at most 4 rows name the same one
- route_weights: float32 [64, 2], P('ep'), may hold values from 0.1 to 1
- expert_gate: bfloat16 [16, 4096, 2048], P('ep', 'tp'), may hold values from -0.09375 to 0.09375
- expert_up: bfloat16 [16, 4096, 2048], P('ep', 'tp'), may hold values from -0.09375 to 0.09375
- expert_down: bfloat16 [16, 2048, 4096], P('ep', None, 'tp'), may hold values from -0.125 to 0.125
- dense_gate: bfloat16 [4096, 2048], P('tp', 'ep'), may hold values from -0.09375 to 0.09375
- dense_up: bfloat16 [4096, 2048], P('tp', 'ep'), may hold values from -0.09375 to 0.09375
- dense_down: bfloat16 [2048, 4096], P('ep', 'tp'), may hold values from -0.25 to 0.25
- dense_mix: bfloat16 [4096], replicated, may hold values from -0.09375 to 0.09375
Outputs:
- layer_out: bfloat16 [64, 4096], P('ep', 'tp')
The draws below stay inside these ranges and needn't reach their ends.
Inputs may be any that keep to these rules, and one draw needn't show every extreme that they name: `lengths`: positions below a sequence's length hold its cache; the new token stands at that position. Some sequence has length 1024 in every draw. `expert_ids`: each row names 2 different experts. Among the rows of one device's 16 sequences (aligned blocks) no expert is named more than 4 times, and in every draw some expert is named exactly 4 times in some block.
All inputs are finite; a program needn't handle non-finite values.
Results may differ from the reference program's by a relative error of at most 0.04.
Values may be sent and summed in bfloat16 or wider, within the bound.
No kernel may reach another device: no remote copies, remote signals or barrier semaphores. Data moves between devices by JAX's collectives and lax.ppermute only.
A program may use at most 128 MiB of HBM per device.

```python
import math
import jax
import jax.numpy as jnp
import numpy as np
from jax import lax

D = 4096
HEADS = 32
KV_HEADS = 16
SUB = 64
VD = 128
EXPERTS = 16
FFE = 2048
FFD = 2048
TOPK = 2
SEQ_DEV = 16
CACHE = 1024
SEQS = 64
CAP = 4


def draw_key_cache(key, part):
    rand_keys = jax.random.split(jax.random.fold_in(key, 11), 1)
    full_shape = (SEQS, CACHE, KV_HEADS, 2 * SUB)
    values = jnp.clip(1.75 * jax.random.normal(rand_keys[0], full_shape, jnp.float32), -10.5, 10.5)
    return values.astype(jnp.bfloat16)


def draw_lengths(key, part):
    rand_keys = jax.random.split(jax.random.fold_in(key, 23), 3)
    group_rate = jax.random.randint(rand_keys[0], (SEQS // SEQ_DEV,), 1, 5)
    seq_rate = jnp.repeat(group_rate, SEQ_DEV)
    shortest = CACHE // 8
    raw_draw = jax.random.randint(rand_keys[1], (SEQS,), 0, CACHE)
    lengths = shortest + raw_draw * seq_rate * (CACHE - shortest) // (4 * CACHE)
    longest = jax.random.randint(rand_keys[2], (), 0, SEQS)
    return jnp.where(jnp.arange(SEQS, dtype=jnp.int32) == longest, CACHE, lengths).astype(jnp.int32)


def draw_first_gain(key, part):
    rand_keys = jax.random.split(jax.random.fold_in(key, 37), 2)
    ramp = jnp.arange(D, dtype=jnp.float32) / (D - 1)
    trend = jnp.exp(jnp.log(0.5) + ramp * (jnp.log(2.0) - jnp.log(0.5)))
    rough = jax.random.uniform(rand_keys[1], (D,), jnp.float32, 0.7, 1.4)
    return (trend * rough).astype(jnp.float32)


def steps_of(key, dims, cuts, least, top_value):
    factor_of = 1.0
    for dim, parts in cuts:
        steps = jax.random.uniform(jax.random.fold_in(jax.random.fold_in(key, 6), dim), (parts,), jnp.float32, least / len(cuts), top_value / len(cuts))
        factor_of = factor_of * jnp.repeat(jnp.exp(steps), dims[dim] // parts).reshape((-1,) + (1,) * (len(dims) - 1 - dim))
    return factor_of


def assign_block(own_key, own, number, rows, count, top, limit, skew):
    ranking = jax.random.permutation(own_key, count)
    heavy_load, usual = portions_of(count, rows * top, limit, skew, True), portions_of(count, rows * top, limit, skew, False)
    places = jnp.arange(count)

    def named(sizes, rotation):
        used = int((sizes > 0).sum())
        fixed = max(1, used // 4)
        passed = fixed + (places - fixed + rotation * (used - fixed)) % max(1, count - fixed)
        return jnp.zeros((count,), jnp.int32).at[ranking[jnp.where(places < fixed, places, passed)]].set(jnp.asarray(sizes, jnp.int32))

    sizes = jnp.where(number % 4 == 0, named(heavy_load, number // 4), named(usual, number - number // 4 - 1))
    mixed = jax.random.permutation(jax.random.fold_in(own, 3), count)
    giver, sink = mixed[0:count // 2 * 2:2], mixed[1:count // 2 * 2:2]
    slack = jnp.minimum(sizes[giver] - 1, limit - sizes[sink]) // 2
    slack = jnp.where((giver == ranking[0]) | (sink == ranking[0]) | (sizes[sink] == 0), 0, jnp.maximum(slack, 0))
    passed = jax.random.randint(jax.random.fold_in(own, 4), (count // 2,), 0, 1 << 20) % (slack + 1)
    sizes = sizes.at[giver].add(-passed).at[sink].add(passed)
    items = jnp.searchsorted(jnp.cumsum(sizes), jnp.arange(rows * top), side="right").astype(jnp.int32)
    table = items.reshape(top, rows).T
    table = table[jax.random.permutation(jax.random.fold_in(own, 1), rows)]
    rotation = jax.random.randint(jax.random.fold_in(own, 2), (rows, 1), 0, top)
    return jnp.take_along_axis(table, (jnp.arange(top)[None, :] + rotation) % top, axis=1)


def portions_of(amount, total, bound, lean, full):
    portions = [(1 << 20) // math.isqrt(rank ** lean) + 1 for rank in range(1, amount + 1)]
    largest = bound if full else min(bound, max(-(-total // amount), total * portions[0] // sum(portions)))
    least = 1 if total - largest >= amount - 1 else 0
    given, rest = [largest] + [least] * (amount - 1), total - largest - least * (amount - 1)
    while rest > 0:
        movable = [i for i in range(1, amount) if given[i] < largest] or [i for i in range(1, amount) if given[i] < bound]
        mass, left = sum([portions[i] for i in movable]), rest
        for i in movable:
            addition = min(bound - given[i], max(1, left * portions[i] // mass), rest)
            given[i] = given[i] + addition
            rest = rest - addition
    return np.array(given)


def centred(rng, shape, scale, bound, cuts=(), kind=jnp.bfloat16):
    drawn = scale * jax.random.normal(rng, shape, jnp.float32)
    if cuts:
        drawn = drawn * steps_of(rng, shape, cuts, -0.22, 0.18)
    return jnp.clip(drawn, -bound, bound).astype(kind)


def setup_inputs(seed: int = 0) -> dict:
    splits = jax.random.split(jax.random.key(seed), 22)
    tokens = centred(splits[0], (SEQS, D), 1.0, 6.0, ((0, 4),))
    query_weight = centred(splits[1], (D, HEADS * 2 * SUB), D ** -0.5, 0.09375, ((0, 4), (1, 8)))
    key_weight = centred(splits[2], (D, KV_HEADS * 2 * SUB), (D // 3) ** -0.5, 0.15625, ((0, 4), (1, 8)))
    value_weight = centred(splits[3], (D, KV_HEADS * VD), D ** -0.5, 0.09375, ((0, 4), (1, 8)))
    out_weight = centred(splits[4], (HEADS * VD, D), (HEADS * VD) ** -0.5, 0.09375, ((0, 8), (1, 4)))
    head_lambda = jnp.clip(0.3 + 0.5 * jax.random.uniform(splits[5], (HEADS,), jnp.float32) ** steps_of(splits[5], (HEADS,), ((0, 8),), -0.2, 0.2), 0.3, 0.8)
    head_gain = jnp.clip(1.0 + 0.18 * jax.random.normal(splits[6], (VD,), jnp.float32), 0.1, 1.9)
    key_cache = draw_key_cache(jax.random.fold_in(splits[21], 71), 0)
    value_cache = centred(splits[8], (SEQS, CACHE, KV_HEADS, VD), 1.0, 6.0, ((0, 4), (2, 8)))
    lengths = draw_lengths(jax.random.fold_in(splits[21], 71), 0)
    first_gain = draw_first_gain(jax.random.fold_in(splits[21], 71), 0)
    second_gain = jnp.clip(1.0 + 0.18 * jax.random.normal(splits[11], (D,), jnp.float32), 0.1, 1.9)
    expert_ids_keys = jax.random.split(jax.random.fold_in(splits[12], 1), SEQS // SEQ_DEV)
    expert_ids_turns = jax.random.permutation(jax.random.fold_in(splits[12], 3), SEQS // SEQ_DEV)
    expert_ids = jax.vmap(lambda own, number: assign_block(jax.random.fold_in(splits[12], 2), own, number, SEQ_DEV, EXPERTS, TOPK, CAP, 2))(expert_ids_keys, expert_ids_turns).reshape((SEQS, TOPK))
    route_weights = jnp.clip(jnp.exp(math.log(1.0) - 2.3025851 * jax.random.uniform(splits[13], (SEQS, TOPK), jnp.float32) ** steps_of(splits[13], (SEQS, TOPK), ((0, 4),), -0.2, 0.2)), 0.1, 1.0)
    expert_gate = centred(splits[14], (EXPERTS, D, FFE), D ** -0.5, 0.09375, ((0, 4), (1, 8)))
    expert_up = centred(splits[15], (EXPERTS, D, FFE), D ** -0.5, 0.09375, ((0, 4), (1, 8)))
    expert_down = centred(splits[16], (EXPERTS, FFE, D), FFE ** -0.5, 0.125, ((0, 4), (2, 8)))
    dense_gate = centred(splits[17], (D, FFD), D ** -0.5, 0.09375, ((0, 8), (1, 4)))
    dense_up = centred(splits[18], (D, FFD), D ** -0.5, 0.09375, ((0, 8), (1, 4)))
    dense_down = centred(splits[19], (FFD, D), (FFD // 4) ** -0.5, 0.25, ((0, 4), (1, 8)))
    dense_mix = centred(splits[20], (D,), D ** -0.5, 0.09375)
    return dict(tokens=tokens, query_weight=query_weight, key_weight=key_weight, value_weight=value_weight, out_weight=out_weight, head_lambda=head_lambda, head_gain=head_gain, key_cache=key_cache, value_cache=value_cache, lengths=lengths, first_gain=first_gain, second_gain=second_gain, expert_ids=expert_ids, route_weights=route_weights, expert_gate=expert_gate, expert_up=expert_up, expert_down=expert_down, dense_gate=dense_gate, dense_up=dense_up, dense_down=dense_down, dense_mix=dense_mix)


theta_base = 500000.0
score_scale = 0.125
head_scale = 0.8
residual_scale = 2.0 ** 0.5
layer_epsilon = 1e-05
head_epsilon = 1e-06

def rotate(vector, cosine, sine_table):
    middle = vector.shape[-1] // 2
    lower = vector[..., :middle]
    upper = vector[..., middle:]
    return jnp.concatenate([lower * cosine - upper * sine_table, upper * cosine + lower * sine_table], axis=-1)

def rounded(array):
    return lax.optimization_barrier(array.astype(jnp.bfloat16)).astype(jnp.float32)

def reference(tokens, query_weight, key_weight, value_weight, out_weight, head_lambda, head_gain, key_cache, value_cache, lengths, first_gain, second_gain, expert_ids, route_weights, expert_gate, expert_up, expert_down, dense_gate, dense_up, dense_down, dense_mix):
    group_size = HEADS // KV_HEADS
    frequency = theta_base ** (-(jnp.arange(SUB // 2, dtype=jnp.float32) * (2.0 / SUB)))
    angles = lengths.astype(jnp.float32)[:, None] * frequency[None, :]
    cosine = jnp.cos(angles)
    sine_table = jnp.sin(angles)
    query_rows = rounded(jnp.dot(tokens, query_weight, preferred_element_type=jnp.float32))
    query_rows = query_rows.reshape(SEQS, KV_HEADS, group_size, 2, SUB)
    query_rows = rounded(rotate(query_rows, cosine[:, None, None, None, :], sine_table[:, None, None, None, :]))
    new_keys = rounded(jnp.dot(tokens, key_weight, preferred_element_type=jnp.float32))
    new_keys = rounded(rotate(new_keys.reshape(SEQS, KV_HEADS, 2, SUB), cosine[:, None, None, :], sine_table[:, None, None, :]))
    new_values = rounded(jnp.dot(tokens, value_weight, preferred_element_type=jnp.float32))
    new_values = new_values.reshape(SEQS, KV_HEADS, VD)
    lambdas = head_lambda.reshape(KV_HEADS, group_size)
    valid = jnp.arange(CACHE, dtype=jnp.int32)[None, :] < lengths[:, None]

    def head_step(head):
        cached_keys = lax.dynamic_index_in_dim(key_cache, head, 2, keepdims=False).astype(jnp.float32)
        cached_keys = cached_keys.reshape(SEQS, CACHE, 2, SUB)
        cached_values = lax.dynamic_index_in_dim(value_cache, head, 2, keepdims=False).astype(jnp.float32)
        head_query = lax.dynamic_index_in_dim(query_rows, head, 1, keepdims=False)
        head_key = lax.dynamic_index_in_dim(new_keys, head, 1, keepdims=False)
        head_value = lax.dynamic_index_in_dim(new_values, head, 1, keepdims=False)
        pair = lax.dynamic_index_in_dim(lambdas, head, 0, keepdims=False)
        scores = jnp.einsum('sgcd,sjcd->sgcj', head_query, cached_keys) * score_scale
        scores = jnp.where(valid[:, None, None, :], scores, -jnp.inf)
        fresh_score = jnp.einsum('sgcd,scd->sgc', head_query, head_key) * score_scale
        highest = jnp.maximum(lax.optimization_barrier(jnp.max(scores, axis=-1)), fresh_score)
        cached_exp = jnp.exp(scores - highest[..., None])
        fresh_exp = jnp.exp(fresh_score - highest)
        denominator = lax.optimization_barrier(jnp.sum(cached_exp, axis=-1)) + fresh_exp
        cached_prob = cached_exp / denominator[..., None]
        fresh_prob = fresh_exp / denominator
        mixed_map = rounded(cached_prob[:, :, 0] - pair[None, :, None] * cached_prob[:, :, 1])
        mixed_new = rounded(fresh_prob[:, :, 0] - pair[None, :] * fresh_prob[:, :, 1])
        return jnp.einsum('sgj,sje->sge', mixed_map, cached_values) + mixed_new[..., None] * head_value[:, None, :]
    head_out = lax.map(head_step, jnp.arange(KV_HEADS, dtype=jnp.int32))
    head_out = jnp.moveaxis(head_out, 0, 1)
    square_mean = lax.optimization_barrier(jnp.mean(head_out * head_out, axis=-1, keepdims=True))
    normed = head_out * lax.rsqrt(square_mean + head_epsilon) * head_gain * head_scale
    normed = normed.astype(jnp.bfloat16).reshape(SEQS, HEADS * VD)
    attention = rounded(jnp.dot(normed, out_weight, preferred_element_type=jnp.float32))
    residual_in = residual_scale * tokens.astype(jnp.float32) + attention
    average = lax.optimization_barrier(jnp.mean(residual_in, axis=-1, keepdims=True))
    centered = residual_in - average
    variance = lax.optimization_barrier(jnp.mean(centered * centered, axis=-1, keepdims=True))
    hidden_in = (centered * lax.rsqrt(variance + layer_epsilon) * first_gain).astype(jnp.bfloat16)
    route_gates = route_weights / lax.optimization_barrier(jnp.sum(route_weights, axis=-1, keepdims=True))

    def expert_step(running, expert):
        gate_matrix = lax.dynamic_index_in_dim(expert_gate, expert, 0, keepdims=False)
        up_matrix = lax.dynamic_index_in_dim(expert_up, expert, 0, keepdims=False)
        down_matrix = lax.dynamic_index_in_dim(expert_down, expert, 0, keepdims=False)
        pre_gate = jnp.dot(hidden_in, gate_matrix, preferred_element_type=jnp.float32)
        pre_up = jnp.dot(hidden_in, up_matrix, preferred_element_type=jnp.float32)
        expert_hidden = (jax.nn.silu(pre_gate) * pre_up).astype(jnp.bfloat16)
        expert_result = rounded(jnp.dot(expert_hidden, down_matrix, preferred_element_type=jnp.float32))
        token_weight = lax.optimization_barrier(jnp.sum(jnp.where(expert_ids == expert, route_gates, 0.0), axis=-1))
        return (running + token_weight[:, None] * expert_result, None)
    expert_mix, _ = lax.scan(expert_step, jnp.zeros((SEQS, D), jnp.float32), jnp.arange(EXPERTS, dtype=jnp.int32))
    dense_pre_gate = jnp.dot(hidden_in, dense_gate, preferred_element_type=jnp.float32)
    dense_pre_up = jnp.dot(hidden_in, dense_up, preferred_element_type=jnp.float32)
    dense_hidden = (jax.nn.silu(dense_pre_gate) * dense_pre_up).astype(jnp.bfloat16)
    dense_out = rounded(jnp.dot(dense_hidden, dense_down, preferred_element_type=jnp.float32))
    mix_gate = jax.nn.sigmoid(jnp.dot(hidden_in, dense_mix, preferred_element_type=jnp.float32))
    combined = residual_scale * hidden_in.astype(jnp.float32) + expert_mix + mix_gate[:, None] * dense_out
    average = lax.optimization_barrier(jnp.mean(combined, axis=-1, keepdims=True))
    variance = lax.optimization_barrier(jnp.mean(combined * combined, axis=-1, keepdims=True)) - average * average
    return ((combined - average) * lax.rsqrt(variance + layer_epsilon) * second_gain).astype(jnp.bfloat16)
```

```python
import jax
import jax.numpy as jnp
from jax import lax
from jax.experimental import pallas as pl
from jax.experimental.pallas import tpu as pltpu
from jax.sharding import PartitionSpec as P

SUB = 64
VD = 128
TOPK = 2
CAP = 4
LANES = 128
CHUNK = 256

theta_base = 500000.0
score_scale = 0.125
head_scale = 0.8
residual_scale = 2.0**0.5
layer_epsilon = 1e-05
head_epsilon = 1e-06

F32 = jnp.float32
BF16 = jnp.bfloat16


def xor_permute(array, axis, count, distance):
    return lax.ppermute(array, axis, [(i, i ^ distance) for i in range(count)])


def attend_kernel(
    lengths_ref,
    qkv_ref,
    cos_ref,
    sin_ref,
    lambda_ref,
    gain_ref,
    keys_ref,
    values_ref,
    out_ref,
    key_buf,
    value_buf,
    query_rows,
    key_rows,
    value_rows,
    score_buf,
    out_rows,
    sems,
    *,
    seq_count,
    kv_local,
    group_size,
    cache,
):
    heads = kv_local * group_size
    chunks = cache // CHUNK
    span = CHUNK * kv_local

    def copy(which, s, c):
        source, target = (keys_ref, key_buf) if which == 0 else (values_ref, value_buf)
        return pltpu.make_async_copy(
            source.at[s, pl.ds(c * span, span)],
            target.at[s, pl.ds(c * span, span)],
            sems.at[which, s, c],
        )

    def start(s, carry):
        for c in range(chunks):

            @pl.when(c * CHUNK < lengths_ref[s])
            def _():
                copy(0, s, c).start()
                copy(1, s, c).start()

        return carry

    lax.fori_loop(0, seq_count, start, 0)

    cosine = cos_ref[...]
    sine = sin_ref[...]
    lane = lax.broadcasted_iota(jnp.int32, (seq_count, LANES), 1)
    low_half = (lane % SUB) < (SUB // 2)
    first_sub = lane < SUB

    def rotated(block):
        swapped = jnp.where(
            low_half, pltpu.roll(block, LANES - SUB // 2, 1), pltpu.roll(block, SUB // 2, 1)
        )
        return (block * cosine + swapped * sine).astype(BF16).astype(F32)

    def column(index):
        return qkv_ref[:, index * LANES : (index + 1) * LANES].astype(F32)

    for h in range(heads):
        turned = rotated(column(h)) * score_scale
        query_rows[:, h, :] = jnp.where(first_sub, turned, 0.0)
        query_rows[:, heads + h, :] = jnp.where(first_sub, 0.0, turned)
    for k in range(kv_local):
        turned = rotated(column(heads + k))
        fresh_value = column(heads + kv_local + k)
        for g in range(group_size):
            key_rows[:, k * group_size + g, :] = turned
            key_rows[:, heads + k * group_size + g, :] = turned
            value_rows[:, k * group_size + g, :] = fresh_value
            value_rows[:, heads + k * group_size + g, :] = fresh_value

    rows = 2 * heads
    row_kv = (lax.broadcasted_iota(jnp.int32, (rows, span), 0) % heads) // group_size
    position = lax.broadcasted_iota(jnp.int32, (rows, span), 1)
    own_kv = (position % kv_local) == row_kv
    position = position // kv_local
    head_weight = lambda_ref[...]

    def one(s, carry):
        length = lengths_ref[s]
        query = query_rows[s]
        fresh = jnp.sum(query * key_rows[s], axis=1, keepdims=True)
        query_low = query.astype(BF16)
        for c in range(chunks):

            @pl.when(c * CHUNK < length)
            def _():
                copy(0, s, c).wait()
                part = lax.dot_general(
                    query_low,
                    key_buf[s, c * span : (c + 1) * span, :],
                    (((1,), (1,)), ((), ())),
                    preferred_element_type=F32,
                )
                taken = own_kv & (position + c * CHUNK < length)
                score_buf[:, c * span : (c + 1) * span] = jnp.where(taken, part, -jnp.inf)

            @pl.when(c * CHUNK >= length)
            def _():
                score_buf[:, c * span : (c + 1) * span] = jnp.full((rows, span), -jnp.inf, F32)

        scores = score_buf[...]
        highest = jnp.maximum(jnp.max(scores, axis=1, keepdims=True), fresh)
        weights = jnp.exp(scores - highest)
        fresh_weight = jnp.exp(fresh - highest)
        total = jnp.sum(weights, axis=1, keepdims=True) + fresh_weight
        factor = head_weight / total
        score_buf[...] = weights * factor
        fresh_part = fresh_weight * factor
        fresh_map = (fresh_part + pltpu.roll(fresh_part, heads, 0)).astype(BF16).astype(F32)
        out_rows[s] = fresh_map * value_rows[s]
        for c in range(chunks):

            @pl.when(c * CHUNK < length)
            def _():
                copy(1, s, c).wait()
                part = score_buf[:, c * span : (c + 1) * span]
                mixed = (part + pltpu.roll(part, heads, 0)).astype(BF16)
                out_rows[s] += jnp.dot(
                    mixed,
                    value_buf[s, c * span : (c + 1) * span, :],
                    preferred_element_type=F32,
                )

        return carry

    lax.fori_loop(0, seq_count, one, 0)
    for h in range(heads):
        head = out_rows[:, h, :]
        square_mean = jnp.mean(head * head, axis=1, keepdims=True)
        normed = head * lax.rsqrt(square_mean + head_epsilon) * gain_ref[...] * head_scale
        out_ref[:, h * LANES : (h + 1) * LANES] = normed.astype(BF16)


def attend(qkv, head_lambda, head_gain, key_cache, value_cache, lengths):
    seq_count, cache, kv_local, _ = key_cache.shape
    heads = head_lambda.shape[0]
    group_size = heads // kv_local
    frequency = theta_base ** (-(jnp.arange(SUB // 2, dtype=F32) * (2.0 / SUB)))
    angles = lengths.astype(F32)[:, None] * frequency[None, :]
    cosine = jnp.cos(angles)
    sine = jnp.sin(angles)
    cosine = jnp.concatenate([cosine] * (2 * LANES // SUB), axis=1)
    sine = jnp.concatenate([-sine, sine] * (LANES // SUB), axis=1)
    weight = jnp.concatenate([jnp.ones_like(head_lambda), -head_lambda])[:, None]
    keys = key_cache.reshape(seq_count, cache * kv_local, 2 * SUB)
    values = value_cache.reshape(seq_count, cache * kv_local, VD)
    rows = 2 * heads
    chunks = cache // CHUNK
    vmem = pl.BlockSpec(memory_space=pltpu.VMEM)
    hbm = pl.BlockSpec(memory_space=pl.ANY)
    return pl.pallas_call(
        lambda *refs: attend_kernel(
            *refs, seq_count=seq_count, kv_local=kv_local, group_size=group_size, cache=cache
        ),
        out_shape=jax.ShapeDtypeStruct((seq_count, heads * VD), BF16),
        in_specs=[pl.BlockSpec(memory_space=pltpu.SMEM), vmem, vmem, vmem, vmem, vmem, hbm, hbm],
        out_specs=vmem,
        scratch_shapes=[
            pltpu.VMEM((seq_count, cache * kv_local, 2 * SUB), BF16),
            pltpu.VMEM((seq_count, cache * kv_local, VD), BF16),
            pltpu.VMEM((seq_count, rows, LANES), F32),
            pltpu.VMEM((seq_count, rows, LANES), F32),
            pltpu.VMEM((seq_count, rows, LANES), F32),
            pltpu.VMEM((rows, cache * kv_local), F32),
            pltpu.VMEM((seq_count, rows, LANES), F32),
            pltpu.SemaphoreType.DMA((2, seq_count, chunks)),
        ],
        compiler_params=pltpu.CompilerParams(vmem_limit_bytes=28 * 1024 * 1024),
        name="attend",
    )(lengths, qkv, cosine, sine, weight, head_gain[None, :], keys, values)


def split_three(array):
    high = array.astype(BF16)
    rest = array - high.astype(F32)
    middle = rest.astype(BF16)
    low = (rest - middle.astype(F32)).astype(BF16)
    return [high, middle, low]


def halves_sum(array, axis, count, distance, dim):
    bit = (lax.axis_index(axis) & distance) != 0
    low, high = jnp.split(array, 2, axis=dim)
    kept = jnp.where(bit, high, low)
    sent = jnp.where(bit, low, high)
    got = xor_permute(sent.astype(BF16), axis, count, distance)
    return kept.astype(F32) + got.astype(F32)


def halves_join(array, axis, count, distance, dim):
    bit = (lax.axis_index(axis) & distance) != 0
    got = xor_permute(array, axis, count, distance)
    return jnp.concatenate(
        [jnp.where(bit, got, array), jnp.where(bit, array, got)], axis=dim
    )


def blocks_xor(array, index, count, dim):
    step = 1
    while step < count:
        size = array.shape[dim] // count
        parts = jnp.split(array, count, axis=dim)
        swapped = jnp.concatenate([parts[b ^ step] for b in range(count)], axis=dim)
        array = jnp.where((index & step) != 0, swapped, array)
        step *= 2
    return array


def doubled_sum(array, axis, count):
    step = 1
    while step < count:
        array = array + xor_permute(array, axis, count, step)
        step *= 2
    return array


def on_device(
    tokens,
    query_weight,
    key_weight,
    value_weight,
    out_weight,
    head_lambda,
    head_gain,
    key_cache,
    value_cache,
    lengths,
    first_gain,
    second_gain,
    expert_ids,
    route_weights,
    expert_gate,
    expert_up,
    expert_down,
    dense_gate,
    dense_up,
    dense_down,
    dense_mix,
):
    seq_count, model_width = tokens.shape
    ep_count = lax.axis_size("ep")
    tp_count = lax.axis_size("tp")
    ep = lax.axis_index("ep")
    tp = lax.axis_index("tp")
    block_width = model_width // ep_count
    slice_width = model_width // tp_count
    local_experts = expert_gate.shape[0]

    extra = jnp.concatenate(
        [expert_ids.astype(BF16)] + split_three(route_weights), axis=1
    )
    extra = jnp.pad(extra, ((0, 0), (0, LANES - extra.shape[1])))

    def piece(distance):
        part = lax.dynamic_slice_in_dim(tokens, (ep ^ distance) * block_width, block_width, 1)
        return jnp.concatenate([part, extra], axis=1)

    pieces = [piece(0)]
    for distance in range(1, ep_count):
        pieces.append(xor_permute(piece(distance), "ep", ep_count, distance))
    arrived = jnp.concatenate(pieces, axis=0)
    columns = arrived[:, :block_width]
    carried = arrived[:, block_width : block_width + 4 * TOPK]
    total_rows = ep_count * seq_count

    projected = jnp.concatenate(
        [
            jnp.dot(columns, query_weight, preferred_element_type=F32),
            jnp.dot(columns, key_weight, preferred_element_type=F32),
            jnp.dot(columns, value_weight, preferred_element_type=F32),
        ],
        axis=1,
    )
    qkv = projected[:seq_count]
    for distance in range(1, ep_count):
        part = projected[distance * seq_count : (distance + 1) * seq_count].astype(BF16)
        qkv = qkv + xor_permute(part, "ep", ep_count, distance).astype(F32)
    normed = attend(
        qkv.astype(BF16), head_lambda, head_gain, key_cache, value_cache, lengths
    )

    all_heads = jnp.concatenate(
        [normed]
        + [xor_permute(normed, "ep", ep_count, distance) for distance in range(1, ep_count)],
        axis=0,
    )
    column_part = jnp.dot(all_heads, out_weight, preferred_element_type=F32).astype(BF16)
    piece_width = block_width // tp_count
    scattered = lax.all_to_all(
        column_part.reshape(total_rows, tp_count, piece_width),
        "tp",
        split_axis=1,
        concat_axis=1,
        tiled=True,
    )
    attention = jnp.sum(scattered.astype(F32), axis=1).astype(BF16)
    own_tokens = lax.dynamic_slice_in_dim(columns, tp * piece_width, piece_width, 1)
    residual = residual_scale * own_tokens.astype(F32) + attention.astype(F32)
    residual = residual.astype(BF16)
    ratio = tp_count // ep_count

    def route(turn):
        pairs = []
        for c in range(ep_count):
            for h in range(ratio):
                for q in range(ep_count):
                    source = c * tp_count + h * ep_count + q
                    pairs.append((source, (q ^ turn) * tp_count + c * ratio + h))
        return pairs

    gathered = jnp.concatenate(
        [lax.ppermute(residual, ("ep", "tp"), route(turn)) for turn in range(ep_count)], axis=1
    )
    gathered = blocks_xor(gathered, ep, ep_count, 1)
    gathered = blocks_xor(gathered, ep ^ (tp // ratio), ep_count, 0).astype(F32)
    moments = doubled_sum(
        jnp.stack([jnp.sum(gathered, axis=1), jnp.sum(gathered * gathered, axis=1)]),
        "tp",
        tp_count,
    )
    average = moments[0] / model_width
    variance = moments[1] / model_width - average * average
    own_gain = lax.dynamic_slice_in_dim(first_gain, tp * slice_width, slice_width, 0)
    hidden = (
        (gathered - average[:, None]) * lax.rsqrt(variance + layer_epsilon)[:, None] * own_gain
    ).astype(BF16)

    ids = carried[:, :TOPK].astype(jnp.int32)
    weights = sum(
        carried[:, TOPK * (i + 1) : TOPK * (i + 2)].astype(F32) for i in range(3)
    )
    gates = weights / jnp.sum(weights, axis=1, keepdims=True)
    pair_count = seq_count * TOPK
    pair_ids = ids.reshape(ep_count, pair_count)
    order = jnp.arange(pair_count, dtype=jnp.int32)
    same = (pair_ids[:, :, None] == pair_ids[:, None, :]) & (order[None, :] < order[:, None])
    rank = jnp.sum(same.astype(jnp.int32), axis=2)
    local = pair_ids - ep * local_experts
    block = jnp.arange(ep_count, dtype=jnp.int32)[:, None]
    slot_count = local_experts * ep_count * CAP
    slot = jnp.where(
        (local >= 0) & (local < local_experts),
        local * (ep_count * CAP) + block * CAP + rank,
        slot_count,
    ).reshape(total_rows, TOPK)
    slots = jnp.arange(slot_count, dtype=jnp.int32)
    hit = slot[:, :, None] == slots[None, None, :]
    placed = jnp.sum(hit.astype(F32), axis=1).astype(BF16)
    combine = jnp.sum(jnp.where(hit, gates[:, :, None], 0.0), axis=1)

    routed = lax.dot_general(
        placed, hidden, (((0,), (0,)), ((), ())), preferred_element_type=F32
    ).astype(BF16)
    routed = routed.reshape(local_experts, ep_count * CAP, slice_width)

    def expert_dot(rows, weight):
        return jnp.einsum("erd,edf->erf", rows, weight, preferred_element_type=F32)

    fold = total_rows // slot_count

    def folded(array):
        return jnp.concatenate(jnp.split(array, fold, axis=0), axis=1)

    def both(expert_weight, dense_weight):
        expert_part = expert_dot(routed, expert_weight).reshape(slot_count, -1)
        dense_part = jnp.dot(hidden, dense_weight, preferred_element_type=F32)
        return jnp.concatenate([expert_part, folded(dense_part)], axis=1)

    pre = jnp.stack([both(expert_gate, dense_gate), both(expert_up, dense_up)])
    distance, dim = 1, 1
    while distance < tp_count:
        pre = halves_sum(pre, "tp", tp_count, distance, dim)
        distance, dim = distance * 2, 2
    active = (jax.nn.silu(pre[0]) * pre[1]).astype(BF16)
    while distance > 1:
        distance //= 2
        active = halves_join(active, "tp", tp_count, distance, 0 if distance == 1 else 1)
    expert_width = expert_gate.shape[2]
    expert_hidden = active[:, :expert_width].reshape(local_experts, ep_count * CAP, expert_width)
    dense_hidden = jnp.concatenate(jnp.split(active[:, expert_width:], fold, axis=1), axis=0)
    result = expert_dot(expert_hidden, expert_down).astype(BF16).reshape(slot_count, slice_width)
    dense_part = jnp.dot(dense_hidden, dense_down, preferred_element_type=F32)

    own_mix = lax.dynamic_slice_in_dim(dense_mix, tp * slice_width, slice_width, 0)
    mix_sum = doubled_sum(
        jnp.sum(hidden.astype(F32) * own_mix.astype(F32), axis=1)[None, :], "tp", tp_count
    )[0]
    mix_gate = jax.nn.sigmoid(mix_sum)
    mixed = jnp.dot(combine, result.astype(F32), precision=lax.Precision.HIGHEST)
    mixed = mixed + mix_gate[:, None] * dense_part
    combined = residual_scale * hidden[:seq_count].astype(F32) + mixed[:seq_count]
    for distance in range(1, ep_count):
        part = mixed[distance * seq_count : (distance + 1) * seq_count].astype(BF16)
        combined = combined + xor_permute(part, "ep", ep_count, distance).astype(F32)
    moments = doubled_sum(
        jnp.stack([jnp.sum(combined, axis=1), jnp.sum(combined * combined, axis=1)]),
        "tp",
        tp_count,
    )
    average = moments[0] / model_width
    variance = moments[1] / model_width - average * average
    layer_out = (
        (combined - average[:, None]) * lax.rsqrt(variance + layer_epsilon)[:, None] * second_gain
    )
    return layer_out.astype(BF16)


def solution(mesh):
    return jax.shard_map(
        on_device,
        mesh=mesh,
        in_specs=(
            P("ep", None),
            P("ep", "tp"),
            P("ep", "tp"),
            P("ep", "tp"),
            P("tp", "ep"),
            P("tp"),
            P(),
            P("ep", None, "tp", None),
            P("ep", None, "tp", None),
            P("ep"),
            P(),
            P("tp"),
            P("ep", None),
            P("ep", None),
            P("ep", "tp", None),
            P("ep", "tp", None),
            P("ep", None, "tp"),
            P("tp", "ep"),
            P("tp", "ep"),
            P("ep", "tp"),
            P(),
        ),
        out_specs=P("ep", "tp"),
        check_vma=False,
    )
```

```python
import functools

import jax
import jax.numpy as jnp
import numpy as np
from jax import lax
from jax.experimental import pallas as pl
from jax.experimental.pallas import tpu as pltpu
from jax.sharding import PartitionSpec as P

SUB = 64
VD = 128
TOPK = 2
CAP = 4
LANES = 128
TAIL = 8
STATS = 4

theta_base = 500000.0
score_scale = 0.125
head_scale = 0.8
residual_scale = 2.0**0.5
layer_epsilon = 1e-05
head_epsilon = 1e-06

F32 = jnp.float32
BF16 = jnp.bfloat16

IN_VMEM = pl.BlockSpec(memory_space=pltpu.VMEM)
IN_SMEM = pl.BlockSpec(memory_space=pltpu.SMEM)


def call(kernel, name, outs, args, scalars=0, scratch=(), mib=4, **sizes):
    return pl.pallas_call(
        functools.partial(kernel, **sizes),
        out_shape=[jax.ShapeDtypeStruct(shape, dtype) for shape, dtype in outs],
        in_specs=[IN_SMEM] * scalars + [IN_VMEM] * (len(args) - scalars),
        out_specs=[IN_VMEM] * len(outs),
        scratch_shapes=[pltpu.VMEM(shape, dtype) for shape, dtype in scratch],
        compiler_params=pltpu.CompilerParams(vmem_limit_bytes=mib * 1024 * 1024),
        name=name,
    )(*args)


def xor_permute(array, axis, count, distance):
    return lax.ppermute(array, axis, [(i, i ^ distance) for i in range(count)])


def xor_all(arrays, axis, count):
    return [xor_permute(arrays[d - 1], axis, count, d) for d in range(1, count)]


def aligned(index, size):
    return pl.ds(pl.multiple_of(index * size, LANES), size)


def iota(shape, dim):
    return lax.broadcasted_iota(jnp.int32, shape, dim)


def row_of(column):
    size = column.shape[0]
    eye = iota((size, size), 0) == iota((size, size), 1)
    return jnp.sum(jnp.where(eye, column, 0.0), axis=0, keepdims=True)


def column_of(row, start, size):
    width = row.shape[1]
    eye = iota((size, width), 0) + start == iota((size, width), 1)
    return jnp.sum(jnp.where(eye, row, 0.0), axis=1, keepdims=True)


def pieces_of(value, count):
    parts = []
    for _ in range(count):
        part = value.astype(BF16).astype(F32)
        parts.append(part)
        value = value - part
    return parts


WEIGHT_LANE = TOPK
MEAN_LANE = WEIGHT_LANE + 3 * TOPK


def prepare_kernel(lengths, tokens, ids, weights, frequency, *outs, ep_count):
    seq_count, width = tokens.shape
    block = width // ep_count
    ep = lax.axis_index("ep")
    lane = iota((seq_count, LANES), 1)
    extra = jnp.zeros((seq_count, LANES), F32)
    fields = []
    for k in range(TOPK):
        fields.append((k, column_of(ids[k : k + 1, :].astype(F32), 0, seq_count)))
        weight = column_of(weights[k : k + 1, :], 0, seq_count)
        for i, part in enumerate(pieces_of(weight, 3)):
            fields.append((WEIGHT_LANE + 3 * k + i, part))
    mean = jnp.sum(tokens[...].astype(F32), axis=1, keepdims=True) * (1.0 / width)
    for i, part in enumerate(pieces_of(mean, 3)):
        fields.append((MEAN_LANE + i, part))
    for place, value in fields:
        extra = jnp.where(lane == place, value, extra)
    extra = extra.astype(BF16)
    for d in range(ep_count):
        outs[d][:, :block] = tokens[:, aligned(ep ^ d, block)]
        outs[d][:, block:] = extra
    row = iota((seq_count, LANES), 0)
    position = jnp.zeros((seq_count, LANES), F32)
    for s in range(seq_count):
        position = jnp.where(row == s, lengths[s].astype(F32), position)
    angle = position * frequency[...]
    low_half = (lane % SUB) < (SUB // 2)
    sine = jnp.sin(angle)
    outs[ep_count][...] = jnp.cos(angle)
    outs[ep_count + 1][...] = jnp.where(low_half, -sine, sine)


def project_kernel(*refs, ep_count):
    pieces, weights, outs = refs[:ep_count], refs[ep_count : ep_count + 3], refs[ep_count + 3 :]
    rows = pieces[0].shape[0]
    block = weights[0].shape[0]
    columns = jnp.concatenate([piece[:, :block] for piece in pieces], axis=0)
    start = 0
    for weight in weights:
        size = weight.shape[1]
        part = jnp.dot(columns, weight[...], preferred_element_type=F32)
        for d in range(ep_count):
            outs[d][:, start : start + size] = part[d * rows : (d + 1) * rows].astype(
                outs[d].dtype
            )
        start += size


def attend_kernel(lengths, lambdas, *refs, ep_count, group):
    sums = refs[:ep_count]
    cos_ref, sin_ref, gain, keys, values, out, query_rows, key_rows, value_rows, out_rows = refs[
        ep_count:
    ]
    seq_count = keys.shape[0]
    heads = lambdas.shape[0]
    kv_local = (sums[0].shape[1] // LANES - heads) // 2
    per_kv = heads // kv_local
    width = keys.shape[1]
    rows = 2 * heads
    cosine = cos_ref[...]
    sine = sin_ref[...]
    lane = iota((seq_count, LANES), 1)
    low_half = (lane % SUB) < (SUB // 2)
    first_sub = lane < SUB

    def column(index):
        place = slice(index * LANES, (index + 1) * LANES)
        total = sums[0][:, place]
        for other in sums[1:]:
            total = total + other[:, place].astype(F32)
        return total.astype(BF16).astype(F32)

    def rotated(block):
        swapped = jnp.where(
            low_half, pltpu.roll(block, LANES - SUB // 2, 1), pltpu.roll(block, SUB // 2, 1)
        )
        return (block * cosine + swapped * sine).astype(BF16).astype(F32)

    for h in range(heads):
        turned = rotated(column(h)) * score_scale
        query_rows[:, h, :] = jnp.where(first_sub, turned, 0.0)
        query_rows[:, heads + h, :] = jnp.where(first_sub, 0.0, turned)
    for k in range(kv_local):
        turned = rotated(column(heads + k))
        fresh_value = column(heads + kv_local + k)
        for g in range(per_kv):
            for place in (k * per_kv + g, heads + k * per_kv + g):
                key_rows[:, place, :] = turned
                value_rows[:, place, :] = fresh_value

    row_kv = (iota((rows, width), 0) % heads) // per_kv
    place = iota((rows, width), 1)
    position = jnp.where((place % kv_local) == row_kv, place // kv_local, width)
    head_row = iota((rows, 1), 0)
    head_weight = jnp.ones((rows, 1), F32)
    for h in range(heads):
        head_weight = jnp.where(head_row == heads + h, -lambdas[h], head_weight)

    def several(step, carry):
        base = step * group
        scores, mixed = [], []
        for u in range(group):
            part = lax.dot_general(
                query_rows[base + u].astype(BF16),
                keys[base + u],
                (((1,), (1,)), ((), ())),
                preferred_element_type=F32,
            )
            scores.append(jnp.where(position < lengths[base + u], part, -jnp.inf))
        for u in range(group):
            fresh = jnp.sum(
                query_rows[base + u] * key_rows[base + u], axis=1, keepdims=True
            )
            highest = jnp.maximum(jnp.max(scores[u], axis=1, keepdims=True), fresh)
            weight = jnp.exp(scores[u] - highest)
            fresh_weight = jnp.exp(fresh - highest)
            factor = head_weight / (jnp.sum(weight, axis=1, keepdims=True) + fresh_weight)
            weight = weight * factor
            fresh_weight = jnp.broadcast_to(fresh_weight * factor, (rows, LANES))
            mixed.append((weight + pltpu.roll(weight, heads, 0)).astype(BF16))
            fresh_weight = fresh_weight + pltpu.roll(fresh_weight, heads, 0)
            out_rows[base + u] = fresh_weight.astype(BF16).astype(F32) * value_rows[base + u]
        for u in range(group):
            out_rows[base + u] += jnp.dot(
                mixed[u], values[base + u], preferred_element_type=F32
            )
        return carry

    lax.fori_loop(0, seq_count // group, several, 0)
    for h in range(heads):
        head = out_rows[:, h, :]
        square_mean = jnp.mean(head * head, axis=1, keepdims=True)
        normed = head * lax.rsqrt(square_mean + head_epsilon) * gain[...] * head_scale
        out[:, h * LANES : (h + 1) * LANES] = normed.astype(BF16)


def out_kernel(*refs, ep_count, ratio):
    heads, weight, outs, full = (
        refs[:ep_count],
        refs[ep_count],
        refs[ep_count + 1 : ep_count + 1 + ratio],
        refs[-1],
    )
    rows = jnp.concatenate([ref[...] for ref in heads], axis=0)
    full[...] = jnp.dot(rows, weight[...], preferred_element_type=F32)
    side = lax.axis_index("tp") % ratio
    size = outs[0].shape[1]
    for d in range(ratio):
        outs[d][...] = full[:, aligned(side ^ d, size)].astype(outs[d].dtype)


def add_kernel(*refs):
    total = refs[0][...].astype(F32)
    for ref in refs[1:-1]:
        total = total + ref[...].astype(F32)
    refs[-1][...] = total.astype(refs[-1].dtype)


def residual_kernel(*refs, ep_count, ratio):
    sums, pieces, out = refs[:ep_count], refs[ep_count : 2 * ep_count], refs[-1]
    rows = pieces[0].shape[0]
    size = out.shape[1]
    side = lax.axis_index("tp") % ratio
    block = pieces[0].shape[1] - LANES
    for d in range(ep_count):
        place = slice(d * rows, (d + 1) * rows)
        total = sums[0][place, :].astype(F32)
        for other in sums[1:]:
            total = total + other[place, :].astype(F32)
        extra = pieces[d][:, block:].astype(F32)
        mean = extra[:, MEAN_LANE : MEAN_LANE + 1]
        for i in range(1, 3):
            mean = mean + extra[:, MEAN_LANE + i : MEAN_LANE + i + 1]
        own = pieces[d][:, aligned(side, size)].astype(F32)
        out[place, :] = (residual_scale * (own - mean) + total).astype(BF16)


def send_part(sent, value):
    rows = value.shape[1]
    sent[:, : rows - STATS, :] = value[:, : rows - STATS, :].astype(BF16)
    sums = value[0, rows - STATS :, :] + value[1, rows - STATS :, :]
    high = sums.astype(BF16)
    sent[0, rows - STATS :, :] = high
    sent[1, rows - STATS :, :] = (sums - high.astype(F32)).astype(BF16)


def experts_kernel(*refs, ep_count, ratio, width):
    own = refs[0]
    arrivals = refs[1:ep_count]
    pieces = refs[ep_count : 2 * ep_count]
    (
        gain_ref,
        mix_ref,
        expert_gate,
        expert_up,
        dense_gate,
        dense_up,
        sent,
        kept,
        placed_out,
        info_out,
        own_out,
        full,
    ) = refs[2 * ep_count :]
    ep = lax.axis_index("ep")
    tp = lax.axis_index("tp")
    seq_count = pieces[0].shape[0]
    total_rows, size = own.shape
    local_experts = expert_gate.shape[0]
    expert_rows = ep_count * CAP
    slot_count = local_experts * expert_rows
    distance = ep ^ (tp // ratio)
    blocks = []
    for i in range(ep_count):
        rows = own[i * seq_count : (i + 1) * seq_count, :].astype(F32)
        rows = jnp.where(distance == 0, rows, 0.0)
        for d in range(1, ep_count):
            j = i ^ d
            rows = rows + arrivals[d - 1][j * seq_count : (j + 1) * seq_count, :].astype(F32)
        blocks.append(rows)
    own_out[...] = blocks[0]
    rows = jnp.concatenate(blocks, axis=0)
    gain = gain_ref[:, aligned(tp, size)]
    mix = mix_ref[:, aligned(tp, size)].astype(F32)
    scaled = rows * gain
    hidden = scaled.astype(BF16)

    block = pieces[0].shape[1] - LANES
    extra = jnp.concatenate([piece[:, block:] for piece in pieces], axis=0).astype(F32)
    token_row = iota((total_rows, total_rows), 0)
    token_lane = iota((total_rows, total_rows), 1)
    earlier = (token_lane < token_row) & (token_lane // seq_count == token_row // seq_count)
    ids = [extra[:, k : k + 1] for k in range(TOPK)]
    id_rows = [row_of(column) for column in ids]
    weights = []
    for k in range(TOPK):
        first = WEIGHT_LANE + 3 * k
        weights.append(
            extra[:, first : first + 1]
            + extra[:, first + 1 : first + 2]
            + extra[:, first + 2 : first + 3]
        )
    weight_sum = weights[0]
    for k in range(1, TOPK):
        weight_sum = weight_sum + weights[k]
    token_block = (iota((total_rows, 1), 0) // seq_count).astype(F32)
    slot_row = iota((slot_count, total_rows), 0).astype(F32)
    placed = jnp.zeros((slot_count, total_rows), F32)
    info = jnp.zeros((total_rows, LANES), F32)
    info_lane = iota((total_rows, LANES), 1)
    first_expert = (ep * local_experts).astype(F32)
    for k in range(TOPK):
        same = jnp.zeros((total_rows, total_rows), F32)
        for other in id_rows:
            same = same + jnp.where(earlier & (ids[k] == other), 1.0, 0.0)
        rank = jnp.sum(same, axis=1, keepdims=True)
        local = ids[k] - first_expert
        slot = local * expert_rows + token_block * CAP + rank
        slot = jnp.where((local >= 0.0) & (local < local_experts), slot, -1.0)
        placed = placed + jnp.where(slot_row == row_of(slot), 1.0, 0.0)
        info = jnp.where(info_lane == k, slot, info)
        info = jnp.where(info_lane == TOPK + k, weights[k] / weight_sum, info)
    info_out[...] = info
    placed_out[...] = placed
    routed = jnp.dot(placed.astype(BF16), hidden, preferred_element_type=F32).astype(BF16)

    sums = [
        jnp.sum(rows, axis=1, keepdims=True),
        jnp.sum(rows * rows, axis=1, keepdims=True),
        jnp.sum(scaled * mix, axis=1, keepdims=True),
        jnp.broadcast_to(jnp.sum(gain * mix, axis=1, keepdims=True), (total_rows, 1)),
    ]
    gain_high = gain.astype(BF16).astype(F32)
    gain_row = iota((16, size), 0)
    gain_rows = jnp.where(
        gain_row == 0, gain_high, jnp.where(gain_row == 1, gain - gain_high, 0.0)
    ).astype(BF16)
    expert_width = expert_gate.shape[2]
    dense_width = dense_gate.shape[1]
    fold = total_rows // slot_count
    full[:, slot_count:, :] = jnp.zeros((2, TAIL, full.shape[2]), F32)
    dense_rows = jnp.concatenate([hidden, gain_rows], axis=0)
    for plane, (expert_weight, dense_weight) in enumerate(
        ((expert_gate, dense_gate), (expert_up, dense_up))
    ):
        for e in range(local_experts):
            lhs = jnp.concatenate(
                [routed[e * expert_rows : (e + 1) * expert_rows], gain_rows], axis=0
            )
            part = jnp.dot(lhs, expert_weight[e], preferred_element_type=F32)
            full[plane, e * expert_rows : (e + 1) * expert_rows, :expert_width] = part[
                :expert_rows
            ]
            full[plane, slot_count + e : slot_count + e + 1, :expert_width] = (
                part[expert_rows : expert_rows + 1] + part[expert_rows + 1 : expert_rows + 2]
            )
        part = jnp.dot(dense_rows, dense_weight[...], preferred_element_type=F32)
        gain_part = part[total_rows : total_rows + 1] + part[total_rows + 1 : total_rows + 2]
        for f in range(fold):
            place = slice(expert_width + f * dense_width, expert_width + (f + 1) * dense_width)
            full[plane, :slot_count, place] = part[f * slot_count : (f + 1) * slot_count]
            for e in range(local_experts):
                full[plane, slot_count + e : slot_count + e + 1, place] = gain_part
    for start in range(0, full.shape[2], width):
        for i in range(STATS):
            at = slot_count + TAIL - STATS + i
            full[0, at : at + 1, start : start + total_rows] = row_of(sums[i])
    half = full.shape[2] // 2
    side = tp & 1
    send_part(sent, full[:, :, aligned(1 - side, half)])
    kept[...] = full[:, :, aligned(side, half)]


def columns_kernel(kept_in, got, sent, kept, full, *, bit):
    full[...] = kept_in[...] + got[...].astype(F32)
    half = full.shape[2] // 2
    side = (lax.axis_index("tp") >> bit) & 1
    send_part(sent, full[:, :, aligned(1 - side, half)])
    kept[...] = full[:, :, aligned(side, half)]


def rows_kernel(kept_in, got, sent, kept, full, *, bit):
    full[...] = kept_in[...] + got[...].astype(F32)
    half = (full.shape[1] - TAIL) // 2
    side = (lax.axis_index("tp") >> bit) & 1
    tail = full[:, 2 * half :, :]
    other = full[:, pl.ds(pl.multiple_of((1 - side) * half, 8), half), :]
    send_part(sent, jnp.concatenate([other, tail], axis=1))
    kept[:, :half, :] = full[:, pl.ds(pl.multiple_of(side * half, 8), half), :]
    kept[:, half:, :] = tail


def act_kernel(
    kept, got, placed, act, stats, *, model_width, expert_width, dense_width, expert_rows, bits
):
    column_bits, row_bits = bits
    total = kept[...] + got[...].astype(F32)
    rows = total.shape[1] - TAIL
    width = total.shape[2]
    slot_count, total_rows = placed.shape
    tp = lax.axis_index("tp")
    sums = total[0, rows + TAIL - STATS :, :] + total[1, rows + TAIL - STATS :, :]
    sums = sums[:, :total_rows]
    mean = sums[0:1] * (1.0 / model_width)
    variance = sums[1:2] * (1.0 / model_width) - mean * mean
    scale = lax.rsqrt(variance + layer_epsilon)
    gate = jax.nn.sigmoid(scale * (sums[2:3] - mean * sums[3:4]))
    stats[0:1, :] = mean
    stats[1:2, :] = scale
    stats[2:3, :] = gate
    first_row = 0
    size = slot_count
    for bit in row_bits:
        size //= 2
        first_row = first_row + ((tp >> bit) & 1) * size
    first_column = 0
    size = expert_width + dense_width * (total_rows // slot_count)
    for bit in column_bits:
        size //= 2
        first_column = first_column + ((tp >> bit) & 1) * size
    mine = placed[pl.ds(pl.multiple_of(first_row, 8), rows), :]
    scale_used = jnp.sum(mine * scale, axis=1, keepdims=True)
    mean_used = jnp.sum(mine * mean, axis=1, keepdims=True)
    column = iota((rows, width), 1) + first_column
    scale_used = jnp.broadcast_to(scale_used, (rows, width))
    mean_used = jnp.broadcast_to(mean_used, (rows, width))
    for f in range(total_rows // slot_count):
        dense = column >= expert_width + f * dense_width
        start = first_row + f * slot_count
        scale_used = jnp.where(dense, column_of(scale, start, rows), scale_used)
        mean_used = jnp.where(dense, column_of(mean, start, rows), mean_used)
    expert = (iota((rows, width), 0) + first_row) // expert_rows
    pre = []
    for plane in range(2):
        gain_sum = jnp.zeros((rows, width), F32)
        for e in range(slot_count // expert_rows):
            gain_sum = jnp.where(expert == e, total[plane, rows + e : rows + e + 1, :], gain_sum)
        pre.append(scale_used * (total[plane, :rows, :] - mean_used * gain_sum))
    act[0] = (pre[0] / (1.0 + jnp.exp(-pre[0])) * pre[1]).astype(BF16)


def down_kernel(
    acts,
    stats,
    info,
    own_rows,
    gain_ref,
    expert_down,
    dense_down,
    *refs,
    ep_count,
    places,
):
    outs, joined = refs[:ep_count], refs[ep_count]
    tp = lax.axis_index("tp")
    piece_rows, piece_width = acts.shape[1:]
    for index, (row, column) in enumerate(places):
        block = acts[index ^ reverse_bits(tp, len(places))]
        joined[row : row + piece_rows, column : column + piece_width] = block
    local_experts, expert_width, size = expert_down.shape
    dense_width = dense_down.shape[0]
    slot_count = joined.shape[0]
    expert_rows = slot_count // local_experts
    total_rows = info.shape[0]
    seq_count = total_rows // ep_count
    results = []
    for e in range(local_experts):
        lhs = joined[e * expert_rows : (e + 1) * expert_rows, :expert_width]
        results.append(jnp.dot(lhs, expert_down[e], preferred_element_type=F32))
    result = jnp.concatenate(results, axis=0).astype(BF16)
    fold = total_rows // slot_count
    dense_rows = jnp.concatenate(
        [
            joined[:, expert_width + f * dense_width : expert_width + (f + 1) * dense_width]
            for f in range(fold)
        ],
        axis=0,
    )
    dense = jnp.dot(dense_rows, dense_down[...], preferred_element_type=F32)
    mixed = column_of(stats[2:3, :], 0, total_rows) * dense
    slot_lane = iota((total_rows, slot_count), 1).astype(F32)
    for k in range(TOPK):
        chosen = jnp.where(info[:, k : k + 1] == slot_lane, 1.0, 0.0).astype(BF16)
        picked = jnp.dot(chosen, result, preferred_element_type=F32)
        mixed = mixed + info[:, TOPK + k : TOPK + k + 1] * picked
    gain = gain_ref[:, aligned(tp, size)]
    mean = column_of(stats[0:1, :], 0, seq_count)
    scale = column_of(stats[1:2, :], 0, seq_count)
    hidden = (own_rows[...] - mean) * scale * gain
    outs[0][...] = mixed[:seq_count] + residual_scale * hidden
    for d in range(1, ep_count):
        outs[d][...] = mixed[d * seq_count : (d + 1) * seq_count].astype(BF16)


def reverse_bits(index, count):
    steps = count.bit_length() - 1
    total = 0
    for step in range(steps):
        total = total + (((index >> step) & 1) << (steps - 1 - step))
    return total


def combine_kernel(*refs):
    combined, moments = refs[-2:]
    total = refs[0][...]
    for ref in refs[1:-2]:
        total = total + ref[...].astype(F32)
    combined[...] = total
    moments[...] = jnp.zeros(moments.shape, F32)
    rows = total.shape[0]
    moments[0:1, :rows] = row_of(jnp.sum(total, axis=1, keepdims=True))
    moments[1:2, :rows] = row_of(jnp.sum(total * total, axis=1, keepdims=True))


def norm_kernel(*refs, model_width):
    combined, gain = refs[0], refs[1]
    out = refs[-1]
    sums = refs[2][...]
    for ref in refs[3:-1]:
        sums = sums + ref[...]
    mean = sums[0:1] * (1.0 / model_width)
    variance = sums[1:2] * (1.0 / model_width) - mean * mean
    rows = combined.shape[0]
    scale = column_of(lax.rsqrt(variance + layer_epsilon), 0, rows)
    out[...] = ((combined[...] - column_of(mean, 0, rows)) * scale * gain[...]).astype(BF16)


def on_device(
    tokens,
    query_weight,
    key_weight,
    value_weight,
    out_weight,
    head_lambda,
    head_gain,
    key_cache,
    value_cache,
    lengths,
    first_gain,
    second_gain,
    expert_ids,
    route_weights,
    expert_gate,
    expert_up,
    expert_down,
    dense_gate,
    dense_up,
    dense_down,
    dense_mix,
):
    seq_count, model_width = tokens.shape
    ep_count = lax.axis_size("ep")
    tp_count = lax.axis_size("tp")
    ratio = tp_count // ep_count
    block_width = model_width // ep_count
    slice_width = model_width // tp_count
    local_experts, _, expert_width = expert_gate.shape
    dense_width = dense_gate.shape[1]
    expert_rows = ep_count * CAP
    slot_count = local_experts * expert_rows
    total_rows = ep_count * seq_count
    heads = head_lambda.shape[0]
    cache, kv_local = key_cache.shape[1:3]

    frequency = theta_base ** (-(np.arange(SUB // 2, dtype=np.float64) * (2.0 / SUB)))
    frequency = np.tile(frequency, LANES // (SUB // 2)).astype(np.float32)[None, :]
    piece = ((seq_count, block_width + LANES), BF16)
    table = ((seq_count, LANES), F32)
    *pieces, cosine, sine = call(
        prepare_kernel,
        "prepare",
        [piece] * ep_count + [table] * 2,
        [lengths, tokens, expert_ids.T, route_weights.T, jnp.asarray(frequency)],
        scalars=1,
        ep_count=ep_count,
    )
    pieces = [pieces[0]] + xor_all(pieces[1:], "ep", ep_count)
    qkv_width = (heads + 2 * kv_local) * LANES
    sums = call(
        project_kernel,
        "project",
        [((seq_count, qkv_width), F32)] + [((seq_count, qkv_width), BF16)] * (ep_count - 1),
        pieces + [query_weight, key_weight, value_weight],
        ep_count=ep_count,
    )
    sums = [sums[0]] + xor_all(sums[1:], "ep", ep_count)
    rows_scratch = ((seq_count, 2 * heads, LANES), F32)
    (normed,) = call(
        attend_kernel,
        "attend",
        [((seq_count, heads * VD), BF16)],
        [lengths, head_lambda]
        + sums
        + [
            cosine,
            sine,
            head_gain[None, :],
            key_cache.reshape(seq_count, cache * kv_local, 2 * SUB),
            value_cache.reshape(seq_count, cache * kv_local, VD),
        ],
        scalars=2,
        scratch=[rows_scratch] * 4,
        ep_count=ep_count,
        group=min(8, seq_count),
    )
    all_heads = [normed] + xor_all([normed] * (ep_count - 1), "ep", ep_count)
    part = (total_rows, slice_width)
    parts = call(
        out_kernel,
        "outproj",
        [(part, F32)] + [(part, BF16)] * (ratio - 1),
        all_heads + [out_weight],
        scratch=[((total_rows, block_width), F32)],
        ep_count=ep_count,
        ratio=ratio,
    )
    parts = [parts[0]] + [
        xor_permute(parts[d], "tp", tp_count, d) for d in range(1, ratio)
    ]
    (part_sum,) = call(add_kernel, "pairsum", [(part, BF16)], parts)

    def device(ep, place, side):
        return ep * tp_count + place * ratio + side

    groups = [(c, h) for c in range(ep_count) for h in range(ratio)]
    both = ("ep", "tp")
    gathered = [part_sum] + [
        lax.ppermute(part_sum, both, [(device(c, c ^ d, h), device(c, c, h)) for c, h in groups])
        for d in range(1, ep_count)
    ]
    (residual,) = call(
        residual_kernel,
        "residual",
        [(part, BF16)],
        gathered + pieces,
        ep_count=ep_count,
        ratio=ratio,
    )
    arrivals = [
        lax.ppermute(residual, both, [(device(c, c, h), device(c ^ d, c, h)) for c, h in groups])
        for d in range(1, ep_count)
    ]

    width = expert_width + dense_width * (total_rows // slot_count)
    column_bits, row_bits = [], []
    piece_width, piece_rows = width, slot_count
    for bit in range(tp_count.bit_length() - 1):
        if piece_width % (2 * LANES) == 0 and not row_bits:
            column_bits.append(bit)
            piece_width //= 2
        else:
            row_bits.append(bit)
            piece_rows //= 2
    full_rows = slot_count + TAIL
    half = (2, full_rows, width // 2)
    sent, kept, placed, info, own_rows = call(
        experts_kernel,
        "experts",
        [
            (half, BF16),
            (half, F32),
            ((slot_count, total_rows), F32),
            ((total_rows, LANES), F32),
            ((seq_count, slice_width), F32),
        ],
        [residual]
        + arrivals
        + pieces
        + [
            first_gain[None, :],
            dense_mix[None, :],
            expert_gate,
            expert_up,
            dense_gate,
            dense_up,
        ],
        scratch=[((2, full_rows, width), F32)],
        mib=8,
        ep_count=ep_count,
        ratio=ratio,
        width=piece_width,
    )
    shape = list(half)
    for bit in range(1, tp_count.bit_length() - 1):
        got = xor_permute(sent, "tp", tp_count, 1 << (bit - 1))
        before = tuple(shape)
        if bit in column_bits:
            shape[2] //= 2
        else:
            shape[1] = (shape[1] - TAIL) // 2 + TAIL
        sent, kept = call(
            columns_kernel if bit in column_bits else rows_kernel,
            "fold%d" % bit,
            [(tuple(shape), BF16), (tuple(shape), F32)],
            [kept, got],
            scratch=[(before, F32)],
            bit=bit,
        )
    got = xor_permute(sent, "tp", tp_count, tp_count // 2)
    act, stats = call(
        act_kernel,
        "act",
        [((1, piece_rows, piece_width), BF16), ((8, total_rows), F32)],
        [kept, got, placed],
        model_width=model_width,
        expert_width=expert_width,
        dense_width=dense_width,
        expert_rows=expert_rows,
        bits=(column_bits, row_bits),
    )
    distance = tp_count // 2
    while distance:
        act = jnp.concatenate([act, xor_permute(act, "tp", tp_count, distance)], axis=0)
        distance //= 2
    steps = tp_count.bit_length() - 1
    places = []
    for index in range(tp_count):
        row, column, rows, columns = 0, 0, slot_count, width
        for bit in range(steps):
            up = (index >> (steps - 1 - bit)) & 1
            if bit in column_bits:
                columns //= 2
                column += up * columns
            else:
                rows //= 2
                row += up * rows
        places.append((row, column))
    mixed = call(
        down_kernel,
        "down",
        [((seq_count, slice_width), F32)]
        + [((seq_count, slice_width), BF16)] * (ep_count - 1),
        [act, stats, info, own_rows, first_gain[None, :], expert_down, dense_down],
        scratch=[((slot_count, width), BF16)],
        ep_count=ep_count,
        places=tuple(places),
    )
    mixed = [mixed[0]] + xor_all(mixed[1:], "ep", ep_count)
    combined, moments = call(
        combine_kernel,
        "combine",
        [((seq_count, slice_width), F32), ((8, LANES), F32)],
        mixed,
    )
    distance = 1
    while distance < tp_count:
        other = xor_permute(moments, "tp", tp_count, distance)
        distance *= 2
        if distance < tp_count:
            moments = moments + other
    (layer_out,) = call(
        norm_kernel,
        "norm",
        [((seq_count, slice_width), BF16)],
        [combined, second_gain[None, :], moments, other],
        model_width=model_width,
    )
    return layer_out


def solution(mesh):
    return jax.shard_map(
        on_device,
        mesh=mesh,
        in_specs=(
            P("ep", None),
            P("ep", "tp"),
            P("ep", "tp"),
            P("ep", "tp"),
            P("tp", "ep"),
            P("tp"),
            P(),
            P("ep", None, "tp", None),
            P("ep", None, "tp", None),
            P("ep"),
            P(),
            P("tp"),
            P("ep", None),
            P("ep", None),
            P("ep", "tp", None),
            P("ep", "tp", None),
            P("ep", None, "tp"),
            P("tp", "ep"),
            P("tp", "ep"),
            P("ep", "tp"),
            P(),
        ),
        out_specs=P("ep", "tp"),
        check_vma=False,
    )
```

```python
import functools
import math

import jax
import jax.numpy as jnp
from jax import lax
from jax.experimental import pallas as pl
from jax.experimental.pallas import tpu as pltpu
from jax.sharding import PartitionSpec as P

SUB = 64
VD = 128
TOPK = 2
CAP = 4
LANES = 128
TAIL = 8
STATS = 4

theta_base = 500000.0
score_scale = 0.125
head_scale = 0.8
residual_scale = 2.0**0.5
layer_epsilon = 1e-05
head_epsilon = 1e-06

F32 = jnp.float32
BF16 = jnp.bfloat16

OVERLAP = 20_000_000_000

IN_VMEM = pl.BlockSpec(memory_space=pltpu.VMEM)
IN_SMEM = pl.BlockSpec(memory_space=pltpu.SMEM)


def call(kernel, name, outs, args, scalars=0, scratch=(), mib=4, cost=0, **sizes):
    return pl.pallas_call(
        functools.partial(kernel, **sizes),
        out_shape=[jax.ShapeDtypeStruct(shape, dtype) for shape, dtype in outs],
        in_specs=[IN_SMEM] * scalars + [IN_VMEM] * (len(args) - scalars),
        out_specs=[IN_VMEM] * len(outs),
        scratch_shapes=[pltpu.VMEM(shape, dtype) for shape, dtype in scratch],
        compiler_params=pltpu.CompilerParams(vmem_limit_bytes=mib * 1024 * 1024),
        cost_estimate=pl.CostEstimate(flops=cost, bytes_accessed=cost, transcendentals=0) if cost else None,
        name=name,
    )(*args)


def xor_permute(array, axis, count, distance):
    return lax.ppermute(array, axis, [(i, i ^ distance) for i in range(count)])


def xor_all(arrays, axis, count):
    return [xor_permute(arrays[d - 1], axis, count, d) for d in range(1, count)]


def places_all(arrays, tp_count):
    got = {}
    order = sorted(range(1, tp_count // 2), key=lambda d: (d != 1, -d))
    for d in order:
        got[d] = xor_permute(arrays[d - 1], "tp", tp_count, 2 * d)
    return [got[d] for d in range(1, tp_count // 2)]


def aligned(index, size):
    return pl.ds(pl.multiple_of(index * size, LANES), size)


def iota(shape, dim):
    return lax.broadcasted_iota(jnp.int32, shape, dim)


def row_of(column):
    size = column.shape[0]
    eye = iota((size, size), 0) == iota((size, size), 1)
    return jnp.sum(jnp.where(eye, column, 0.0), axis=0, keepdims=True)


def column_of(row, start, size):
    width = row.shape[1]
    eye = iota((size, width), 0) + start == iota((size, width), 1)
    return jnp.sum(jnp.where(eye, row, 0.0), axis=1, keepdims=True)


def pieces_of(value, count):
    parts = []
    for _ in range(count):
        part = value.astype(BF16).astype(F32)
        parts.append(part)
        value = value - part
    return parts


WEIGHT_LANE = TOPK
MEAN_LANE = WEIGHT_LANE + 3 * TOPK


def prepare_kernel(tokens, ids, weights, *outs, ep_count):
    seq_count, width = tokens.shape
    block = width // ep_count
    ep = lax.axis_index("ep")
    lane = iota((seq_count, LANES), 1)
    extra = jnp.zeros((seq_count, LANES), F32)
    fields = []
    for k in range(TOPK):
        fields.append((k, column_of(ids[k : k + 1, :].astype(F32), 0, seq_count)))
        weight = column_of(weights[k : k + 1, :], 0, seq_count)
        for i, part in enumerate(pieces_of(weight, 3)):
            fields.append((WEIGHT_LANE + 3 * k + i, part))
    mean = jnp.sum(tokens[...].astype(F32), axis=1, keepdims=True) * (1.0 / width)
    for i, part in enumerate(pieces_of(mean, 3)):
        fields.append((MEAN_LANE + i, part))
    for place, value in fields:
        extra = jnp.where(lane == place, value, extra)
    extra = extra.astype(BF16)
    for d in range(ep_count):
        outs[d][:, :block] = tokens[:, aligned(ep ^ d, block)]
        outs[d][:, block:] = extra


def tables_kernel(lengths, cos_ref, sin_ref):
    seq_count = cos_ref.shape[0]
    lane = iota((seq_count, LANES), 1)
    row = iota((seq_count, LANES), 0)
    position = jnp.zeros((seq_count, LANES), F32)
    for s in range(seq_count):
        position = jnp.where(row == s, lengths[s].astype(F32), position)
    rate = (lane % (SUB // 2)).astype(F32) * (-2.0 / SUB * math.log(theta_base))
    angle = position * jnp.exp(rate)
    low_half = (lane % SUB) < (SUB // 2)
    sine = jnp.sin(angle)
    cos_ref[...] = jnp.cos(angle)
    sin_ref[...] = jnp.where(low_half, -sine, sine)


def project_kernel(*refs, ep_count):
    pieces, weights, outs = refs[:ep_count], refs[ep_count : ep_count + 3], refs[ep_count + 3 :]
    rows = pieces[0].shape[0]
    block = weights[0].shape[0]
    columns = jnp.concatenate([piece[:, :block] for piece in pieces], axis=0)
    start = 0
    for weight in weights:
        size = weight.shape[1]
        part = jnp.dot(columns, weight[...], preferred_element_type=F32)
        for d in range(ep_count):
            outs[d][:, start : start + size] = part[d * rows : (d + 1) * rows].astype(
                outs[d].dtype
            )
        start += size


def attend_kernel(lengths, lambdas, *refs, ep_count, group):
    sums = refs[:ep_count]
    cos_ref, sin_ref, gain, keys, values, out, query_rows, key_rows, value_rows, out_rows = refs[
        ep_count:
    ]
    seq_count = keys.shape[0]
    heads = lambdas.shape[0]
    kv_local = (sums[0].shape[1] // LANES - heads) // 2
    per_kv = heads // kv_local
    width = keys.shape[1]
    rows = 2 * heads
    cosine = cos_ref[...]
    sine = sin_ref[...]
    lane = iota((seq_count, LANES), 1)
    low_half = (lane % SUB) < (SUB // 2)
    first_sub = lane < SUB

    def column(index):
        place = slice(index * LANES, (index + 1) * LANES)
        total = sums[0][:, place]
        for other in sums[1:]:
            total = total + other[:, place].astype(F32)
        return total.astype(BF16).astype(F32)

    def rotated(block):
        swapped = jnp.where(
            low_half, pltpu.roll(block, LANES - SUB // 2, 1), pltpu.roll(block, SUB // 2, 1)
        )
        return (block * cosine + swapped * sine).astype(BF16).astype(F32)

    for h in range(heads):
        turned = rotated(column(h)) * score_scale
        query_rows[:, h, :] = jnp.where(first_sub, turned, 0.0)
        query_rows[:, heads + h, :] = jnp.where(first_sub, 0.0, turned)
    for k in range(kv_local):
        turned = rotated(column(heads + k))
        fresh_value = column(heads + kv_local + k)
        for g in range(per_kv):
            for place in (k * per_kv + g, heads + k * per_kv + g):
                key_rows[:, place, :] = turned
                value_rows[:, place, :] = fresh_value

    row_kv = (iota((rows, width), 0) % heads) // per_kv
    place = iota((rows, width), 1)
    position = jnp.where((place % kv_local) == row_kv, place // kv_local, width)
    head_row = iota((rows, 1), 0)
    head_weight = jnp.ones((rows, 1), F32)
    for h in range(heads):
        head_weight = jnp.where(head_row == heads + h, -lambdas[h], head_weight)

    def several(step, carry):
        base = step * group
        scores, mixed = [], []
        for u in range(group):
            part = lax.dot_general(
                query_rows[base + u].astype(BF16),
                keys[base + u],
                (((1,), (1,)), ((), ())),
                preferred_element_type=F32,
            )
            scores.append(jnp.where(position < lengths[base + u], part, -jnp.inf))
        for u in range(group):
            fresh = jnp.sum(
                query_rows[base + u] * key_rows[base + u], axis=1, keepdims=True
            )
            highest = jnp.maximum(jnp.max(scores[u], axis=1, keepdims=True), fresh)
            weight = jnp.exp(scores[u] - highest)
            fresh_weight = jnp.exp(fresh - highest)
            factor = head_weight / (jnp.sum(weight, axis=1, keepdims=True) + fresh_weight)
            weight = weight * factor
            fresh_weight = jnp.broadcast_to(fresh_weight * factor, (rows, LANES))
            mixed.append((weight + pltpu.roll(weight, heads, 0)).astype(BF16))
            fresh_weight = fresh_weight + pltpu.roll(fresh_weight, heads, 0)
            out_rows[base + u] = fresh_weight.astype(BF16).astype(F32) * value_rows[base + u]
        for u in range(group):
            out_rows[base + u] += jnp.dot(
                mixed[u], values[base + u], preferred_element_type=F32
            )
        return carry

    lax.fori_loop(0, seq_count // group, several, 0)
    for h in range(heads):
        head = out_rows[:, h, :]
        square_mean = jnp.mean(head * head, axis=1, keepdims=True)
        normed = head * lax.rsqrt(square_mean + head_epsilon) * gain[...] * head_scale
        out[:, h * LANES : (h + 1) * LANES] = normed.astype(BF16)


def out_kernel(*refs, ep_count, ratio):
    heads, weight, outs, full = (
        refs[:ep_count],
        refs[ep_count],
        refs[ep_count + 1 : ep_count + 1 + ratio],
        refs[-1],
    )
    rows = jnp.concatenate([ref[...] for ref in heads], axis=0)
    full[...] = jnp.dot(rows, weight[...], preferred_element_type=F32)
    side = lax.axis_index("tp") % ratio
    size = outs[0].shape[1]
    for d in range(ratio):
        outs[d][...] = full[:, aligned(side ^ d, size)].astype(outs[d].dtype)


def add_kernel(*refs):
    total = refs[0][...].astype(F32)
    for ref in refs[1:-1]:
        total = total + ref[...].astype(F32)
    refs[-1][...] = total.astype(refs[-1].dtype)


def residual_kernel(*refs, ep_count, ratio):
    sums, pieces, out = refs[:ep_count], refs[ep_count : 2 * ep_count], refs[-1]
    rows = pieces[0].shape[0]
    size = out.shape[1]
    side = lax.axis_index("tp") % ratio
    block = pieces[0].shape[1] - LANES
    for d in range(ep_count):
        place = slice(d * rows, (d + 1) * rows)
        total = sums[0][place, :].astype(F32)
        for other in sums[1:]:
            total = total + other[place, :].astype(F32)
        extra = pieces[d][:, block:].astype(F32)
        mean = extra[:, MEAN_LANE : MEAN_LANE + 1]
        for i in range(1, 3):
            mean = mean + extra[:, MEAN_LANE + i : MEAN_LANE + i + 1]
        own = pieces[d][:, aligned(side, size)].astype(F32)
        out[place, :] = (residual_scale * (own - mean) + total).astype(BF16)


def send_part(sent, value):
    rows = value.shape[1]
    sent[:, : rows - STATS, :] = value[:, : rows - STATS, :].astype(BF16)
    sums = value[0, rows - STATS :, :] + value[1, rows - STATS :, :]
    high = sums.astype(BF16)
    sent[0, rows - STATS :, :] = high
    sent[1, rows - STATS :, :] = (sums - high.astype(F32)).astype(BF16)


def experts_kernel(*refs, ep_count, ratio, width):
    own = refs[0]
    arrivals = refs[1:ep_count]
    pieces = refs[ep_count : 2 * ep_count]
    (
        gain_ref,
        mix_ref,
        expert_gate,
        expert_up,
        dense_gate,
        dense_up,
        sent,
        kept,
        placed_out,
        info_out,
        own_out,
        full,
    ) = refs[2 * ep_count :]
    ep = lax.axis_index("ep")
    tp = lax.axis_index("tp")
    seq_count = pieces[0].shape[0]
    total_rows, size = own.shape
    local_experts = expert_gate.shape[0]
    expert_rows = ep_count * CAP
    slot_count = local_experts * expert_rows
    distance = ep ^ (tp // ratio)
    blocks = []
    for i in range(ep_count):
        rows = own[i * seq_count : (i + 1) * seq_count, :].astype(F32)
        rows = jnp.where(distance == 0, rows, 0.0)
        for d in range(1, ep_count):
            j = i ^ d
            rows = rows + arrivals[d - 1][j * seq_count : (j + 1) * seq_count, :].astype(F32)
        blocks.append(rows)
    own_out[...] = blocks[0]
    rows = jnp.concatenate(blocks, axis=0)
    gain = gain_ref[:, aligned(tp, size)]
    mix = mix_ref[:, aligned(tp, size)].astype(F32)
    scaled = rows * gain
    hidden = scaled.astype(BF16)

    block = pieces[0].shape[1] - LANES
    extra = jnp.concatenate([piece[:, block:] for piece in pieces], axis=0).astype(F32)
    token_row = iota((total_rows, total_rows), 0)
    token_lane = iota((total_rows, total_rows), 1)
    earlier = (token_lane < token_row) & (token_lane // seq_count == token_row // seq_count)
    ids = [extra[:, k : k + 1] for k in range(TOPK)]
    id_rows = [row_of(column) for column in ids]
    weights = []
    for k in range(TOPK):
        first = WEIGHT_LANE + 3 * k
        weights.append(
            extra[:, first : first + 1]
            + extra[:, first + 1 : first + 2]
            + extra[:, first + 2 : first + 3]
        )
    weight_sum = weights[0]
    for k in range(1, TOPK):
        weight_sum = weight_sum + weights[k]
    token_block = (iota((total_rows, 1), 0) // seq_count).astype(F32)
    slot_row = iota((slot_count, total_rows), 0).astype(F32)
    placed = jnp.zeros((slot_count, total_rows), F32)
    info = jnp.zeros((total_rows, LANES), F32)
    info_lane = iota((total_rows, LANES), 1)
    first_expert = (ep * local_experts).astype(F32)
    for k in range(TOPK):
        same = jnp.zeros((total_rows, total_rows), F32)
        for other in id_rows:
            same = same + jnp.where(earlier & (ids[k] == other), 1.0, 0.0)
        rank = jnp.sum(same, axis=1, keepdims=True)
        local = ids[k] - first_expert
        slot = local * expert_rows + token_block * CAP + rank
        slot = jnp.where((local >= 0.0) & (local < local_experts), slot, -1.0)
        placed = placed + jnp.where(slot_row == row_of(slot), 1.0, 0.0)
        info = jnp.where(info_lane == k, slot, info)
        info = jnp.where(info_lane == TOPK + k, weights[k] / weight_sum, info)
    info_out[...] = info
    placed_out[...] = placed
    routed = jnp.dot(placed.astype(BF16), hidden, preferred_element_type=F32).astype(BF16)

    sums = [
        jnp.sum(rows, axis=1, keepdims=True),
        jnp.sum(rows * rows, axis=1, keepdims=True),
        jnp.sum(scaled * mix, axis=1, keepdims=True),
        jnp.broadcast_to(jnp.sum(gain * mix, axis=1, keepdims=True), (total_rows, 1)),
    ]
    gain_high = gain.astype(BF16).astype(F32)
    gain_row = iota((16, size), 0)
    gain_rows = jnp.where(
        gain_row == 0, gain_high, jnp.where(gain_row == 1, gain - gain_high, 0.0)
    ).astype(BF16)
    expert_width = expert_gate.shape[2]
    dense_width = dense_gate.shape[1]
    fold = total_rows // slot_count
    full[:, slot_count:, :] = jnp.zeros((2, TAIL, full.shape[2]), F32)
    dense_rows = jnp.concatenate([hidden, gain_rows], axis=0)
    for plane, (expert_weight, dense_weight) in enumerate(
        ((expert_gate, dense_gate), (expert_up, dense_up))
    ):
        for e in range(local_experts):
            lhs = jnp.concatenate(
                [routed[e * expert_rows : (e + 1) * expert_rows], gain_rows], axis=0
            )
            part = jnp.dot(lhs, expert_weight[e], preferred_element_type=F32)
            full[plane, e * expert_rows : (e + 1) * expert_rows, :expert_width] = part[
                :expert_rows
            ]
            full[plane, slot_count + e : slot_count + e + 1, :expert_width] = (
                part[expert_rows : expert_rows + 1] + part[expert_rows + 1 : expert_rows + 2]
            )
        part = jnp.dot(dense_rows, dense_weight[...], preferred_element_type=F32)
        gain_part = part[total_rows : total_rows + 1] + part[total_rows + 1 : total_rows + 2]
        for f in range(fold):
            place = slice(expert_width + f * dense_width, expert_width + (f + 1) * dense_width)
            full[plane, :slot_count, place] = part[f * slot_count : (f + 1) * slot_count]
            for e in range(local_experts):
                full[plane, slot_count + e : slot_count + e + 1, place] = gain_part
    for start in range(0, full.shape[2], width):
        for i in range(STATS):
            at = slot_count + TAIL - STATS + i
            full[0, at : at + 1, start : start + total_rows] = row_of(sums[i])
    half = full.shape[2] // 2
    side = tp & 1
    send_part(sent, full[:, :, aligned(1 - side, half)])
    kept[...] = full[:, :, aligned(side, half)]


def piece_at(index, bits, rows, width):
    row, column = 0, 0
    for bit, splits_columns in enumerate(bits):
        up = (index >> bit) & 1
        if splits_columns:
            width //= 2
            column = column + up * width
        else:
            rows //= 2
            row = row + up * rows
    return row, column


def spread_kernel(kept, got, *refs, bits):
    outs, full = refs[:-1], refs[-1]
    full[...] = kept[...] + got[...].astype(F32)
    rows = full.shape[1] - TAIL
    piece_rows = outs[0].shape[1] - TAIL
    width = outs[0].shape[2]
    place = lax.axis_index("tp") >> 1
    for d, out in enumerate(outs):
        row, column = piece_at(place ^ d, bits, rows, full.shape[2])
        lanes = pl.ds(pl.multiple_of(column, LANES), width)
        main = full[:, pl.ds(pl.multiple_of(row, 8), piece_rows), lanes]
        tail = full[:, rows:, lanes]
        if d == 0:
            out[:, :piece_rows, :] = main
            out[:, piece_rows:, :] = tail
        else:
            send_part(out, jnp.concatenate([main, tail], axis=1))


def act_kernel(
    *refs, model_width, expert_width, dense_width, expert_rows, bits
):
    placed, act, stats = refs[-3:]
    total = refs[0][...]
    for ref in refs[1:-3]:
        total = total + ref[...].astype(F32)
    rows = total.shape[1] - TAIL
    width = total.shape[2]
    slot_count, total_rows = placed.shape
    tp = lax.axis_index("tp")
    sums = total[0, rows + TAIL - STATS :, :] + total[1, rows + TAIL - STATS :, :]
    sums = sums[:, :total_rows]
    mean = sums[0:1] * (1.0 / model_width)
    variance = sums[1:2] * (1.0 / model_width) - mean * mean
    scale = lax.rsqrt(variance + layer_epsilon)
    gate = jax.nn.sigmoid(scale * (sums[2:3] - mean * sums[3:4]))
    stats[0:1, :] = mean
    stats[1:2, :] = scale
    stats[2:3, :] = gate
    whole = expert_width + dense_width * (total_rows // slot_count)
    first_row, first_column = piece_at(tp >> 1, bits, slot_count, whole // 2)
    first_column = first_column + (tp & 1) * (whole // 2)
    mine = placed[pl.ds(pl.multiple_of(first_row, 8), rows), :]
    scale_used = jnp.sum(mine * scale, axis=1, keepdims=True)
    mean_used = jnp.sum(mine * mean, axis=1, keepdims=True)
    column = iota((rows, width), 1) + first_column
    scale_used = jnp.broadcast_to(scale_used, (rows, width))
    mean_used = jnp.broadcast_to(mean_used, (rows, width))
    for f in range(total_rows // slot_count):
        dense = column >= expert_width + f * dense_width
        start = first_row + f * slot_count
        scale_used = jnp.where(dense, column_of(scale, start, rows), scale_used)
        mean_used = jnp.where(dense, column_of(mean, start, rows), mean_used)
    expert = (iota((rows, width), 0) + first_row) // expert_rows
    pre = []
    for plane in range(2):
        gain_sum = jnp.zeros((rows, width), F32)
        for e in range(slot_count // expert_rows):
            gain_sum = jnp.where(expert == e, total[plane, rows + e : rows + e + 1, :], gain_sum)
        pre.append(scale_used * (total[plane, :rows, :] - mean_used * gain_sum))
    act[0] = (pre[0] / (1.0 + jnp.exp(-pre[0])) * pre[1]).astype(BF16)


def down_kernel(
    acts,
    stats,
    info,
    own_rows,
    gain_ref,
    expert_down,
    dense_down,
    *refs,
    ep_count,
    places,
):
    outs, joined = refs[:ep_count], refs[ep_count]
    tp = lax.axis_index("tp")
    piece_rows, piece_width = acts.shape[1:]
    for index, (row, column) in enumerate(places):
        block = acts[index ^ ((tp & 1) * (len(places) // 2) + (tp >> 1))]
        joined[row : row + piece_rows, column : column + piece_width] = block
    local_experts, expert_width, size = expert_down.shape
    dense_width = dense_down.shape[0]
    slot_count = joined.shape[0]
    expert_rows = slot_count // local_experts
    total_rows = info.shape[0]
    seq_count = total_rows // ep_count
    results = []
    for e in range(local_experts):
        lhs = joined[e * expert_rows : (e + 1) * expert_rows, :expert_width]
        results.append(jnp.dot(lhs, expert_down[e], preferred_element_type=F32))
    result = jnp.concatenate(results, axis=0).astype(BF16)
    fold = total_rows // slot_count
    dense_rows = jnp.concatenate(
        [
            joined[:, expert_width + f * dense_width : expert_width + (f + 1) * dense_width]
            for f in range(fold)
        ],
        axis=0,
    )
    dense = jnp.dot(dense_rows, dense_down[...], preferred_element_type=F32)
    mixed = column_of(stats[2:3, :], 0, total_rows) * dense
    slot_lane = iota((total_rows, slot_count), 1).astype(F32)
    for k in range(TOPK):
        chosen = jnp.where(info[:, k : k + 1] == slot_lane, 1.0, 0.0).astype(BF16)
        picked = jnp.dot(chosen, result, preferred_element_type=F32)
        mixed = mixed + info[:, TOPK + k : TOPK + k + 1] * picked
    gain = gain_ref[:, aligned(tp, size)]
    mean = column_of(stats[0:1, :], 0, seq_count)
    scale = column_of(stats[1:2, :], 0, seq_count)
    hidden = (own_rows[...] - mean) * scale * gain
    outs[0][...] = mixed[:seq_count] + residual_scale * hidden
    for d in range(1, ep_count):
        outs[d][...] = mixed[d * seq_count : (d + 1) * seq_count].astype(BF16)


def combine_kernel(*refs):
    combined, moments = refs[-2:]
    total = refs[0][...]
    for ref in refs[1:-2]:
        total = total + ref[...].astype(F32)
    combined[...] = total
    moments[...] = jnp.zeros(moments.shape, F32)
    rows = total.shape[0]
    moments[0:1, :rows] = row_of(jnp.sum(total, axis=1, keepdims=True))
    moments[1:2, :rows] = row_of(jnp.sum(total * total, axis=1, keepdims=True))


def norm_kernel(*refs, model_width):
    combined, gain = refs[0], refs[1]
    out = refs[-1]
    sums = refs[2][...]
    for ref in refs[3:-1]:
        sums = sums + ref[...]
    mean = sums[0:1] * (1.0 / model_width)
    variance = sums[1:2] * (1.0 / model_width) - mean * mean
    rows = combined.shape[0]
    scale = column_of(lax.rsqrt(variance + layer_epsilon), 0, rows)
    out[...] = ((combined[...] - column_of(mean, 0, rows)) * scale * gain[...]).astype(BF16)


def on_device(
    tokens,
    query_weight,
    key_weight,
    value_weight,
    out_weight,
    head_lambda,
    head_gain,
    key_cache,
    value_cache,
    lengths,
    first_gain,
    second_gain,
    expert_ids,
    route_weights,
    expert_gate,
    expert_up,
    expert_down,
    dense_gate,
    dense_up,
    dense_down,
    dense_mix,
):
    seq_count, model_width = tokens.shape
    ep_count = lax.axis_size("ep")
    tp_count = lax.axis_size("tp")
    ratio = tp_count // ep_count
    block_width = model_width // ep_count
    slice_width = model_width // tp_count
    local_experts, _, expert_width = expert_gate.shape
    dense_width = dense_gate.shape[1]
    expert_rows = ep_count * CAP
    slot_count = local_experts * expert_rows
    total_rows = ep_count * seq_count
    heads = head_lambda.shape[0]
    cache, kv_local = key_cache.shape[1:3]

    piece = ((seq_count, block_width + LANES), BF16)
    table = ((seq_count, LANES), F32)
    pieces = call(
        prepare_kernel,
        "prepare",
        [piece] * ep_count,
        [
            pltpu.with_memory_space_constraint(array, pltpu.HBM)
            for array in (tokens, expert_ids.T, route_weights.T)
        ],
        cost=OVERLAP,
        ep_count=ep_count,
    )
    cosine, sine = call(tables_kernel, "tables", [table] * 2, [lengths], scalars=1)
    pieces = [pieces[0]] + xor_all(pieces[1:], "ep", ep_count)
    qkv_width = (heads + 2 * kv_local) * LANES
    sums = call(
        project_kernel,
        "project",
        [((seq_count, qkv_width), F32)] + [((seq_count, qkv_width), BF16)] * (ep_count - 1),
        pieces + [query_weight, key_weight, value_weight],
        ep_count=ep_count,
    )
    sums = [sums[0]] + xor_all(sums[1:], "ep", ep_count)
    rows_scratch = ((seq_count, 2 * heads, LANES), F32)
    (normed,) = call(
        attend_kernel,
        "attend",
        [((seq_count, heads * VD), BF16)],
        [lengths, head_lambda]
        + sums
        + [
            cosine,
            sine,
            head_gain[None, :],
            key_cache.reshape(seq_count, cache * kv_local, 2 * SUB),
            value_cache.reshape(seq_count, cache * kv_local, VD),
        ],
        scalars=2,
        scratch=[rows_scratch] * 4,
        cost=OVERLAP,
        ep_count=ep_count,
        group=min(8, seq_count),
    )
    all_heads = [normed] + xor_all([normed] * (ep_count - 1), "ep", ep_count)
    part = (total_rows, slice_width)
    parts = call(
        out_kernel,
        "outproj",
        [(part, F32)] + [(part, BF16)] * (ratio - 1),
        all_heads + [out_weight],
        scratch=[((total_rows, block_width), F32)],
        ep_count=ep_count,
        ratio=ratio,
    )
    parts = [parts[0]] + [
        xor_permute(parts[d], "tp", tp_count, d) for d in range(1, ratio)
    ]
    (part_sum,) = call(add_kernel, "pairsum", [(part, BF16)], parts)

    def device(ep, place, side):
        return ep * tp_count + place * ratio + side

    groups = [(c, h) for c in range(ep_count) for h in range(ratio)]
    both = ("ep", "tp")
    gathered = [part_sum] + [
        lax.ppermute(part_sum, both, [(device(c, c ^ d, h), device(c, c, h)) for c, h in groups])
        for d in range(1, ep_count)
    ]
    (residual,) = call(
        residual_kernel,
        "residual",
        [(part, BF16)],
        gathered + pieces,
        ep_count=ep_count,
        ratio=ratio,
    )
    arrivals = [
        lax.ppermute(residual, both, [(device(c, c, h), device(c ^ d, c, h)) for c, h in groups])
        for d in range(1, ep_count)
    ]

    width = expert_width + dense_width * (total_rows // slot_count)
    place_count = tp_count // 2
    bits = []
    piece_width, piece_rows = width // 2, slot_count
    for _ in range(place_count.bit_length() - 1):
        bits.append(piece_width % (2 * LANES) == 0)
        if bits[-1]:
            piece_width //= 2
        else:
            piece_rows //= 2
    bits = tuple(bits)
    full_rows = slot_count + TAIL
    half = (2, full_rows, width // 2)
    sent, kept, placed, info, own_rows = call(
        experts_kernel,
        "experts",
        [
            (half, BF16),
            (half, F32),
            ((slot_count, total_rows), F32),
            ((total_rows, LANES), F32),
            ((seq_count, slice_width), F32),
        ],
        [residual]
        + arrivals
        + pieces
        + [
            first_gain[None, :],
            dense_mix[None, :],
            expert_gate,
            expert_up,
            dense_gate,
            dense_up,
        ],
        scratch=[((2, full_rows, width), F32)],
        mib=8,
        ep_count=ep_count,
        ratio=ratio,
        width=piece_width,
    )
    got = xor_permute(sent, "tp", tp_count, 1)
    piece = (2, piece_rows + TAIL, piece_width)
    parts = call(
        spread_kernel,
        "spread",
        [(piece, F32)] + [(piece, BF16)] * (place_count - 1),
        [kept, got],
        scratch=[(half, F32)],
        bits=bits,
    )
    parts = [parts[0]] + places_all(parts[1:], tp_count)
    act, stats = call(
        act_kernel,
        "act",
        [((1, piece_rows, piece_width), BF16), ((8, total_rows), F32)],
        parts + [placed],
        model_width=model_width,
        expert_width=expert_width,
        dense_width=dense_width,
        expert_rows=expert_rows,
        bits=bits,
    )
    act = jnp.concatenate([act] + places_all([act] * (place_count - 1), tp_count), axis=0)
    act = jnp.concatenate([act, xor_permute(act, "tp", tp_count, 1)], axis=0)
    places = []
    for index in range(tp_count):
        row, column = piece_at(index % place_count, bits, slot_count, width // 2)
        places.append((row, column + index // place_count * (width // 2)))
    mixed = call(
        down_kernel,
        "down",
        [((seq_count, slice_width), F32)]
        + [((seq_count, slice_width), BF16)] * (ep_count - 1),
        [act, stats, info, own_rows, first_gain[None, :], expert_down, dense_down],
        scratch=[((slot_count, width), BF16)],
        ep_count=ep_count,
        places=tuple(places),
    )
    mixed = [mixed[0]] + xor_all(mixed[1:], "ep", ep_count)
    combined, moments = call(
        combine_kernel,
        "combine",
        [((seq_count, slice_width), F32), ((8, LANES), F32)],
        mixed,
    )
    moments = moments + xor_permute(moments, "tp", tp_count, 1)
    others = places_all([moments] * (place_count - 1), tp_count)
    (layer_out,) = call(
        norm_kernel,
        "norm",
        [((seq_count, slice_width), BF16)],
        [combined, second_gain[None, :], moments] + others,
        model_width=model_width,
    )
    return layer_out


def solution(mesh):
    return jax.shard_map(
        on_device,
        mesh=mesh,
        in_specs=(
            P("ep", None),
            P("ep", "tp"),
            P("ep", "tp"),
            P("ep", "tp"),
            P("tp", "ep"),
            P("tp"),
            P(),
            P("ep", None, "tp", None),
            P("ep", None, "tp", None),
            P("ep"),
            P(),
            P("tp"),
            P("ep", None),
            P("ep", None),
            P("ep", "tp", None),
            P("ep", "tp", None),
            P("ep", None, "tp"),
            P("tp", "ep"),
            P("tp", "ep"),
            P("ep", "tp"),
            P(),
        ),
        out_specs=P("ep", "tp"),
        check_vma=False,
    )
```

```python
import functools
import math

import jax
import jax.numpy as jnp
from jax import lax
from jax.experimental import pallas as pl
from jax.experimental.pallas import tpu as pltpu
from jax.sharding import PartitionSpec as P

SUB = 64
VD = 128
TOPK = 2
CAP = 4
LANES = 128
TAIL = 8
STATS = 4

theta_base = 500000.0
score_scale = 0.125
head_scale = 0.8
residual_scale = 2.0**0.5
layer_epsilon = 1e-05
head_epsilon = 1e-06

F32 = jnp.float32
BF16 = jnp.bfloat16

OVERLAP = 20_000_000_000

IN_VMEM = pl.BlockSpec(memory_space=pltpu.VMEM)
IN_SMEM = pl.BlockSpec(memory_space=pltpu.SMEM)


def call(kernel, name, outs, args, scalars=0, scratch=(), mib=4, cost=0, **sizes):
    return pl.pallas_call(
        functools.partial(kernel, **sizes),
        out_shape=[jax.ShapeDtypeStruct(shape, dtype) for shape, dtype in outs],
        in_specs=[IN_SMEM] * scalars + [IN_VMEM] * (len(args) - scalars),
        out_specs=[IN_VMEM] * len(outs),
        scratch_shapes=[pltpu.VMEM(shape, dtype) for shape, dtype in scratch],
        compiler_params=pltpu.CompilerParams(vmem_limit_bytes=mib * 1024 * 1024),
        cost_estimate=pl.CostEstimate(flops=cost, bytes_accessed=cost, transcendentals=0) if cost else None,
        name=name,
    )(*args)


def xor_permute(array, axis, count, distance):
    return lax.ppermute(array, axis, [(i, i ^ distance) for i in range(count)])


def xor_all(arrays, axis, count):
    return [xor_permute(arrays[d - 1], axis, count, d) for d in range(1, count)]


def places_all(arrays, tp_count):
    got = {}
    order = sorted(range(1, tp_count // 2), key=lambda d: (d != 1, -d))
    for d in order:
        got[d] = xor_permute(arrays[d - 1], "tp", tp_count, 2 * d)
    return [got[d] for d in range(1, tp_count // 2)]


def aligned(index, size):
    return pl.ds(pl.multiple_of(index * size, LANES), size)


def iota(shape, dim):
    return lax.broadcasted_iota(jnp.int32, shape, dim)


def row_of(column):
    size = column.shape[0]
    eye = iota((size, size), 0) == iota((size, size), 1)
    return jnp.sum(jnp.where(eye, column, 0.0), axis=0, keepdims=True)


def column_of(row, start, size):
    width = row.shape[1]
    eye = iota((size, width), 0) + start == iota((size, width), 1)
    return jnp.sum(jnp.where(eye, row, 0.0), axis=1, keepdims=True)


def pieces_of(value, count):
    parts = []
    for _ in range(count):
        part = value.astype(BF16).astype(F32)
        parts.append(part)
        value = value - part
    return parts


WEIGHT_LANE = TOPK
MEAN_LANE = WEIGHT_LANE + 3 * TOPK


def prepare_kernel(tokens, ids, weights, *outs, ep_count):
    seq_count, width = tokens.shape
    block = width // ep_count
    ep = lax.axis_index("ep")
    lane = iota((seq_count, LANES), 1)
    extra = jnp.zeros((seq_count, LANES), F32)
    fields = []
    for k in range(TOPK):
        fields.append((k, column_of(ids[k : k + 1, :].astype(F32), 0, seq_count)))
        weight = column_of(weights[k : k + 1, :], 0, seq_count)
        for i, part in enumerate(pieces_of(weight, 3)):
            fields.append((WEIGHT_LANE + 3 * k + i, part))
    mean = jnp.sum(tokens[...].astype(F32), axis=1, keepdims=True) * (1.0 / width)
    for i, part in enumerate(pieces_of(mean, 3)):
        fields.append((MEAN_LANE + i, part))
    for place, value in fields:
        extra = jnp.where(lane == place, value, extra)
    extra = extra.astype(BF16)
    for d in range(ep_count):
        outs[d][:, :block] = tokens[:, aligned(ep ^ d, block)]
        outs[d][:, block:] = extra


def tables_kernel(lengths, cos_ref, sin_ref):
    seq_count = cos_ref.shape[0]
    lane = iota((seq_count, LANES), 1)
    row = iota((seq_count, LANES), 0)
    position = jnp.zeros((seq_count, LANES), F32)
    for s in range(seq_count):
        position = jnp.where(row == s, lengths[s].astype(F32), position)
    rate = (lane % (SUB // 2)).astype(F32) * (-2.0 / SUB * math.log(theta_base))
    angle = position * jnp.exp(rate)
    low_half = (lane % SUB) < (SUB // 2)
    sine = jnp.sin(angle)
    cos_ref[...] = jnp.cos(angle)
    sin_ref[...] = jnp.where(low_half, -sine, sine)


def project_kernel(*refs, ep_count):
    pieces, weights, outs = refs[:ep_count], refs[ep_count : ep_count + 3], refs[ep_count + 3 :]
    rows = pieces[0].shape[0]
    block = weights[0].shape[0]
    columns = jnp.concatenate([piece[:, :block] for piece in pieces], axis=0)
    start = 0
    for weight in weights:
        size = weight.shape[1]
        part = jnp.dot(columns, weight[...], preferred_element_type=F32)
        for d in range(ep_count):
            outs[d][:, start : start + size] = part[d * rows : (d + 1) * rows].astype(
                outs[d].dtype
            )
        start += size


def attend_kernel(lengths, lambdas, *refs, ep_count, group):
    sums = refs[:ep_count]
    cos_ref, sin_ref, gain, keys, values, out, query_rows, key_rows, value_rows, out_rows = refs[
        ep_count:
    ]
    seq_count = keys.shape[0]
    heads = lambdas.shape[0]
    kv_local = (sums[0].shape[1] // LANES - heads) // 2
    per_kv = heads // kv_local
    width = keys.shape[1]
    rows = 2 * heads
    cosine = cos_ref[...]
    sine = sin_ref[...]
    lane = iota((seq_count, LANES), 1)
    low_half = (lane % SUB) < (SUB // 2)
    first_sub = lane < SUB

    def column(index):
        place = slice(index * LANES, (index + 1) * LANES)
        total = sums[0][:, place]
        for other in sums[1:]:
            total = total + other[:, place].astype(F32)
        return total.astype(BF16).astype(F32)

    def rotated(block):
        swapped = jnp.where(
            low_half, pltpu.roll(block, LANES - SUB // 2, 1), pltpu.roll(block, SUB // 2, 1)
        )
        return (block * cosine + swapped * sine).astype(BF16).astype(F32)

    for h in range(heads):
        turned = rotated(column(h)) * score_scale
        query_rows[:, h, :] = jnp.where(first_sub, turned, 0.0)
        query_rows[:, heads + h, :] = jnp.where(first_sub, 0.0, turned)
    for k in range(kv_local):
        turned = rotated(column(heads + k))
        fresh_value = column(heads + kv_local + k)
        for g in range(per_kv):
            for place in (k * per_kv + g, heads + k * per_kv + g):
                key_rows[:, place, :] = turned
                value_rows[:, place, :] = fresh_value

    row_kv = (iota((rows, width), 0) % heads) // per_kv
    place = iota((rows, width), 1)
    position = jnp.where((place % kv_local) == row_kv, place // kv_local, width)
    head_row = iota((rows, 1), 0)
    head_weight = jnp.ones((rows, 1), F32)
    for h in range(heads):
        head_weight = jnp.where(head_row == heads + h, -lambdas[h], head_weight)

    def several(step, carry):
        base = step * group
        scores, mixed = [], []
        for u in range(group):
            part = lax.dot_general(
                query_rows[base + u].astype(BF16),
                keys[base + u],
                (((1,), (1,)), ((), ())),
                preferred_element_type=F32,
            )
            scores.append(jnp.where(position < lengths[base + u], part, -jnp.inf))
        for u in range(group):
            fresh = jnp.sum(
                query_rows[base + u] * key_rows[base + u], axis=1, keepdims=True
            )
            highest = jnp.maximum(jnp.max(scores[u], axis=1, keepdims=True), fresh)
            weight = jnp.exp(scores[u] - highest)
            fresh_weight = jnp.exp(fresh - highest)
            factor = head_weight / (jnp.sum(weight, axis=1, keepdims=True) + fresh_weight)
            weight = weight * factor
            fresh_weight = jnp.broadcast_to(fresh_weight * factor, (rows, LANES))
            mixed.append((weight + pltpu.roll(weight, heads, 0)).astype(BF16))
            fresh_weight = fresh_weight + pltpu.roll(fresh_weight, heads, 0)
            out_rows[base + u] = fresh_weight.astype(BF16).astype(F32) * value_rows[base + u]
        for u in range(group):
            out_rows[base + u] += jnp.dot(
                mixed[u], values[base + u], preferred_element_type=F32
            )
        return carry

    lax.fori_loop(0, seq_count // group, several, 0)
    for h in range(heads):
        head = out_rows[:, h, :]
        square_mean = jnp.mean(head * head, axis=1, keepdims=True)
        normed = head * lax.rsqrt(square_mean + head_epsilon) * gain[...] * head_scale
        out[:, h * LANES : (h + 1) * LANES] = normed.astype(BF16)


def out_kernel(*refs, ep_count, ratio):
    heads, weight, outs, full = (
        refs[:ep_count],
        refs[ep_count],
        refs[ep_count + 1 : ep_count + 1 + ratio],
        refs[-1],
    )
    rows = jnp.concatenate([ref[...] for ref in heads], axis=0)
    full[...] = jnp.dot(rows, weight[...], preferred_element_type=F32)
    side = lax.axis_index("tp") % ratio
    size = outs[0].shape[1]
    for d in range(ratio):
        outs[d][...] = full[:, aligned(side ^ d, size)].astype(outs[d].dtype)


def add_kernel(*refs):
    total = refs[0][...].astype(F32)
    for ref in refs[1:-1]:
        total = total + ref[...].astype(F32)
    refs[-1][...] = total.astype(refs[-1].dtype)


def residual_kernel(*refs, ep_count, ratio):
    sums, pieces, out = refs[:ep_count], refs[ep_count : 2 * ep_count], refs[-1]
    rows = pieces[0].shape[0]
    size = out.shape[1]
    side = lax.axis_index("tp") % ratio
    block = pieces[0].shape[1] - LANES
    for d in range(ep_count):
        place = slice(d * rows, (d + 1) * rows)
        total = sums[0][place, :].astype(F32)
        for other in sums[1:]:
            total = total + other[place, :].astype(F32)
        extra = pieces[d][:, block:].astype(F32)
        mean = extra[:, MEAN_LANE : MEAN_LANE + 1]
        for i in range(1, 3):
            mean = mean + extra[:, MEAN_LANE + i : MEAN_LANE + i + 1]
        own = pieces[d][:, aligned(side, size)].astype(F32)
        out[place, :] = (residual_scale * (own - mean) + total).astype(BF16)


def send_part(sent, value):
    rows = value.shape[1]
    sent[:, : rows - STATS, :] = value[:, : rows - STATS, :].astype(BF16)
    sums = value[0, rows - STATS :, :] + value[1, rows - STATS :, :]
    high = sums.astype(BF16)
    sent[0, rows - STATS :, :] = high
    sent[1, rows - STATS :, :] = (sums - high.astype(F32)).astype(BF16)


def routing_kernel(*refs, ep_count, local_experts):
    pieces, placed_out, info_out = refs[:ep_count], refs[-2], refs[-1]
    ep = lax.axis_index("ep")
    seq_count = pieces[0].shape[0]
    slot_count, total_rows = placed_out.shape
    expert_rows = ep_count * CAP

    block = pieces[0].shape[1] - LANES
    extra = jnp.concatenate([piece[:, block:] for piece in pieces], axis=0).astype(F32)
    token_row = iota((total_rows, total_rows), 0)
    token_lane = iota((total_rows, total_rows), 1)
    earlier = (token_lane < token_row) & (token_lane // seq_count == token_row // seq_count)
    ids = [extra[:, k : k + 1] for k in range(TOPK)]
    id_rows = [row_of(column) for column in ids]
    weights = []
    for k in range(TOPK):
        first = WEIGHT_LANE + 3 * k
        weights.append(
            extra[:, first : first + 1]
            + extra[:, first + 1 : first + 2]
            + extra[:, first + 2 : first + 3]
        )
    weight_sum = weights[0]
    for k in range(1, TOPK):
        weight_sum = weight_sum + weights[k]
    token_block = (iota((total_rows, 1), 0) // seq_count).astype(F32)
    slot_row = iota((slot_count, total_rows), 0).astype(F32)
    placed = jnp.zeros((slot_count, total_rows), F32)
    info = jnp.zeros((total_rows, LANES), F32)
    info_lane = iota((total_rows, LANES), 1)
    first_expert = (ep * local_experts).astype(F32)
    for k in range(TOPK):
        same = jnp.zeros((total_rows, total_rows), F32)
        for other in id_rows:
            same = same + jnp.where(earlier & (ids[k] == other), 1.0, 0.0)
        rank = jnp.sum(same, axis=1, keepdims=True)
        local = ids[k] - first_expert
        slot = local * expert_rows + token_block * CAP + rank
        slot = jnp.where((local >= 0.0) & (local < local_experts), slot, -1.0)
        placed = placed + jnp.where(slot_row == row_of(slot), 1.0, 0.0)
        info = jnp.where(info_lane == k, slot, info)
        info = jnp.where(info_lane == TOPK + k, weights[k] / weight_sum, info)
    info_out[...] = info
    placed_out[...] = placed


def experts_kernel(*refs, ep_count, ratio, width):
    own = refs[0]
    arrivals = refs[1:ep_count]
    (
        placed,
        gain_ref,
        mix_ref,
        expert_gate,
        expert_up,
        dense_gate,
        dense_up,
        sent,
        kept,
        own_out,
        full,
    ) = refs[ep_count:]
    ep = lax.axis_index("ep")
    tp = lax.axis_index("tp")
    total_rows, size = own.shape
    seq_count = total_rows // ep_count
    local_experts = expert_gate.shape[0]
    expert_rows = ep_count * CAP
    slot_count = local_experts * expert_rows
    distance = ep ^ (tp // ratio)
    blocks = []
    for i in range(ep_count):
        rows = own[i * seq_count : (i + 1) * seq_count, :].astype(F32)
        rows = jnp.where(distance == 0, rows, 0.0)
        for d in range(1, ep_count):
            j = i ^ d
            rows = rows + arrivals[d - 1][j * seq_count : (j + 1) * seq_count, :].astype(F32)
        blocks.append(rows)
    own_out[...] = blocks[0]
    rows = jnp.concatenate(blocks, axis=0)
    gain = gain_ref[:, aligned(tp, size)]
    mix = mix_ref[:, aligned(tp, size)].astype(F32)
    scaled = rows * gain
    hidden = scaled.astype(BF16)

    routed = jnp.dot(placed[...].astype(BF16), hidden, preferred_element_type=F32).astype(BF16)

    sums = [
        jnp.sum(rows, axis=1, keepdims=True),
        jnp.sum(rows * rows, axis=1, keepdims=True),
        jnp.sum(scaled * mix, axis=1, keepdims=True),
        jnp.broadcast_to(jnp.sum(gain * mix, axis=1, keepdims=True), (total_rows, 1)),
    ]
    gain_high = gain.astype(BF16).astype(F32)
    gain_row = iota((16, size), 0)
    gain_rows = jnp.where(
        gain_row == 0, gain_high, jnp.where(gain_row == 1, gain - gain_high, 0.0)
    ).astype(BF16)
    expert_width = expert_gate.shape[2]
    dense_width = dense_gate.shape[1]
    fold = total_rows // slot_count
    full[:, slot_count:, :] = jnp.zeros((2, TAIL, full.shape[2]), F32)
    dense_rows = jnp.concatenate([hidden, gain_rows], axis=0)
    for plane, (expert_weight, dense_weight) in enumerate(
        ((expert_gate, dense_gate), (expert_up, dense_up))
    ):
        for e in range(local_experts):
            lhs = jnp.concatenate(
                [routed[e * expert_rows : (e + 1) * expert_rows], gain_rows], axis=0
            )
            part = jnp.dot(lhs, expert_weight[e], preferred_element_type=F32)
            full[plane, e * expert_rows : (e + 1) * expert_rows, :expert_width] = part[
                :expert_rows
            ]
            full[plane, slot_count + e : slot_count + e + 1, :expert_width] = (
                part[expert_rows : expert_rows + 1] + part[expert_rows + 1 : expert_rows + 2]
            )
        part = jnp.dot(dense_rows, dense_weight[...], preferred_element_type=F32)
        gain_part = part[total_rows : total_rows + 1] + part[total_rows + 1 : total_rows + 2]
        for f in range(fold):
            place = slice(expert_width + f * dense_width, expert_width + (f + 1) * dense_width)
            full[plane, :slot_count, place] = part[f * slot_count : (f + 1) * slot_count]
            for e in range(local_experts):
                full[plane, slot_count + e : slot_count + e + 1, place] = gain_part
    for start in range(0, full.shape[2], width):
        for i in range(STATS):
            at = slot_count + TAIL - STATS + i
            full[0, at : at + 1, start : start + total_rows] = row_of(sums[i])
    half = full.shape[2] // 2
    side = tp & 1
    send_part(sent, full[:, :, aligned(1 - side, half)])
    kept[...] = full[:, :, aligned(side, half)]


def piece_at(index, bits, rows, width):
    row, column = 0, 0
    for bit, splits_columns in enumerate(bits):
        up = (index >> bit) & 1
        if splits_columns:
            width //= 2
            column = column + up * width
        else:
            rows //= 2
            row = row + up * rows
    return row, column


def low_lane(total_rows):
    return -(-total_rows // LANES) * LANES


def spread_kernel(kept, got, *refs, bits, expert_rows, total_rows):
    outs, full, tail = refs[:-2], refs[-2], refs[-1]
    full[...] = kept[...] + got[...].astype(F32)
    slot_count = full.shape[1] - TAIL
    width = outs[0].shape[1]
    piece_rows = (outs[0].shape[0] - tail.shape[0]) // 2
    experts = max(1, piece_rows // expert_rows)
    place = lax.axis_index("tp") >> 1
    low = low_lane(total_rows)
    for d, out in enumerate(outs):
        row, column = piece_at(place ^ d, bits, slot_count, full.shape[2])
        lanes = pl.ds(pl.multiple_of(column, LANES), width)
        first = slot_count + row // expert_rows
        tail[...] = jnp.zeros(tail.shape, F32)
        for plane in range(2):
            main = full[plane, pl.ds(pl.multiple_of(row, 8), piece_rows), lanes]
            out[plane * piece_rows : (plane + 1) * piece_rows, :] = main.astype(out.dtype)
            for i in range(experts):
                at = plane * experts + i
                tail[at : at + 1, :] = full[plane, pl.ds(first + i, 1), lanes]
        sums = full[:, slot_count + TAIL - STATS :, lanes]
        sums = (sums[0] + sums[1])[:, :total_rows]
        rows = slice(2 * experts, 2 * experts + STATS)
        if d:
            high = sums.astype(BF16).astype(F32)
            tail[rows, :total_rows] = high
            tail[rows, low : low + total_rows] = sums - high
        else:
            tail[rows, :total_rows] = sums
        out[2 * piece_rows :, :] = tail[...].astype(out.dtype)


def act_kernel(
    *refs, model_width, expert_width, dense_width, expert_rows, bits
):
    placed, act, stats = refs[-3:]
    total = refs[0][...]
    for ref in refs[1:-3]:
        total = total + ref[...].astype(F32)
    rows, width = act.shape[1:]
    slot_count, total_rows = placed.shape
    experts = max(1, rows // expert_rows)
    tp = lax.axis_index("tp")
    low = low_lane(total_rows)
    sums = total[2 * (rows + experts) : 2 * (rows + experts) + STATS, :]
    sums = sums[:, :total_rows] + sums[:, low : low + total_rows]
    mean = sums[0:1] * (1.0 / model_width)
    variance = sums[1:2] * (1.0 / model_width) - mean * mean
    scale = lax.rsqrt(variance + layer_epsilon)
    gate = jax.nn.sigmoid(scale * (sums[2:3] - mean * sums[3:4]))
    stats[0:1, :] = mean
    stats[1:2, :] = scale
    stats[2:3, :] = gate
    whole = expert_width + dense_width * (total_rows // slot_count)
    first_row, first_column = piece_at(tp >> 1, bits, slot_count, whole // 2)
    first_column = first_column + (tp & 1) * (whole // 2)
    mine = placed[pl.ds(pl.multiple_of(first_row, 8), rows), :]
    scale_used = jnp.sum(mine * scale, axis=1, keepdims=True)
    mean_used = jnp.sum(mine * mean, axis=1, keepdims=True)
    column = iota((rows, width), 1) + first_column
    scale_used = jnp.broadcast_to(scale_used, (rows, width))
    mean_used = jnp.broadcast_to(mean_used, (rows, width))
    for f in range(total_rows // slot_count):
        dense = column >= expert_width + f * dense_width
        start = first_row + f * slot_count
        scale_used = jnp.where(dense, column_of(scale, start, rows), scale_used)
        mean_used = jnp.where(dense, column_of(mean, start, rows), mean_used)
    expert = iota((rows, width), 0) // expert_rows
    pre = []
    for plane in range(2):
        gain_sum = jnp.zeros((rows, width), F32)
        for i in range(experts):
            at = 2 * rows + plane * experts + i
            gain_sum = jnp.where(expert == i, total[at : at + 1, :], gain_sum)
        main = total[plane * rows : (plane + 1) * rows, :]
        pre.append(scale_used * (main - mean_used * gain_sum))
    act[0] = (pre[0] / (1.0 + jnp.exp(-pre[0])) * pre[1]).astype(BF16)


def down_kernel(
    acts,
    stats,
    info,
    own_rows,
    gain_ref,
    expert_down,
    dense_down,
    *refs,
    ep_count,
    places,
):
    outs, joined = refs[:ep_count], refs[ep_count]
    tp = lax.axis_index("tp")
    piece_rows, piece_width = acts.shape[1:]
    for index, (row, column) in enumerate(places):
        block = acts[index ^ ((tp & 1) * (len(places) // 2) + (tp >> 1))]
        joined[row : row + piece_rows, column : column + piece_width] = block
    local_experts, expert_width, size = expert_down.shape
    dense_width = dense_down.shape[0]
    slot_count = joined.shape[0]
    expert_rows = slot_count // local_experts
    total_rows = info.shape[0]
    seq_count = total_rows // ep_count
    results = []
    for e in range(local_experts):
        lhs = joined[e * expert_rows : (e + 1) * expert_rows, :expert_width]
        results.append(jnp.dot(lhs, expert_down[e], preferred_element_type=F32))
    result = jnp.concatenate(results, axis=0).astype(BF16)
    fold = total_rows // slot_count
    dense_rows = jnp.concatenate(
        [
            joined[:, expert_width + f * dense_width : expert_width + (f + 1) * dense_width]
            for f in range(fold)
        ],
        axis=0,
    )
    dense = jnp.dot(dense_rows, dense_down[...], preferred_element_type=F32)
    mixed = column_of(stats[2:3, :], 0, total_rows) * dense
    slot_lane = iota((total_rows, slot_count), 1).astype(F32)
    for k in range(TOPK):
        chosen = jnp.where(info[:, k : k + 1] == slot_lane, 1.0, 0.0).astype(BF16)
        picked = jnp.dot(chosen, result, preferred_element_type=F32)
        mixed = mixed + info[:, TOPK + k : TOPK + k + 1] * picked
    gain = gain_ref[:, aligned(tp, size)]
    mean = column_of(stats[0:1, :], 0, seq_count)
    scale = column_of(stats[1:2, :], 0, seq_count)
    hidden = (own_rows[...] - mean) * scale * gain
    outs[0][...] = mixed[:seq_count] + residual_scale * hidden
    for d in range(1, ep_count):
        outs[d][...] = mixed[d * seq_count : (d + 1) * seq_count].astype(BF16)


def combine_kernel(*refs):
    combined, moments = refs[-2:]
    total = refs[0][...]
    for ref in refs[1:-2]:
        total = total + ref[...].astype(F32)
    combined[...] = total
    moments[...] = jnp.zeros(moments.shape, F32)
    rows = total.shape[0]
    moments[0:1, :rows] = row_of(jnp.sum(total, axis=1, keepdims=True))
    moments[1:2, :rows] = row_of(jnp.sum(total * total, axis=1, keepdims=True))


def norm_kernel(*refs, model_width):
    combined, gain = refs[0], refs[1]
    out = refs[-1]
    sums = refs[2][...]
    for ref in refs[3:-1]:
        sums = sums + ref[...]
    mean = sums[0:1] * (1.0 / model_width)
    variance = sums[1:2] * (1.0 / model_width) - mean * mean
    rows = combined.shape[0]
    scale = column_of(lax.rsqrt(variance + layer_epsilon), 0, rows)
    out[...] = ((combined[...] - column_of(mean, 0, rows)) * scale * gain[...]).astype(BF16)


def on_device(
    tokens,
    query_weight,
    key_weight,
    value_weight,
    out_weight,
    head_lambda,
    head_gain,
    key_cache,
    value_cache,
    lengths,
    first_gain,
    second_gain,
    expert_ids,
    route_weights,
    expert_gate,
    expert_up,
    expert_down,
    dense_gate,
    dense_up,
    dense_down,
    dense_mix,
):
    seq_count, model_width = tokens.shape
    ep_count = lax.axis_size("ep")
    tp_count = lax.axis_size("tp")
    ratio = tp_count // ep_count
    block_width = model_width // ep_count
    slice_width = model_width // tp_count
    local_experts, _, expert_width = expert_gate.shape
    dense_width = dense_gate.shape[1]
    expert_rows = ep_count * CAP
    slot_count = local_experts * expert_rows
    total_rows = ep_count * seq_count
    heads = head_lambda.shape[0]
    cache, kv_local = key_cache.shape[1:3]

    piece = ((seq_count, block_width + LANES), BF16)
    table = ((seq_count, LANES), F32)
    pieces = call(
        prepare_kernel,
        "prepare",
        [piece] * ep_count,
        [
            pltpu.with_memory_space_constraint(array, pltpu.HBM)
            for array in (tokens, expert_ids.T, route_weights.T)
        ],
        cost=OVERLAP,
        ep_count=ep_count,
    )
    cosine, sine = call(tables_kernel, "tables", [table] * 2, [lengths], scalars=1)
    pieces = [pieces[0]] + xor_all(pieces[1:], "ep", ep_count)
    qkv_width = (heads + 2 * kv_local) * LANES
    sums = call(
        project_kernel,
        "project",
        [((seq_count, qkv_width), F32)] + [((seq_count, qkv_width), BF16)] * (ep_count - 1),
        pieces + [query_weight, key_weight, value_weight],
        ep_count=ep_count,
    )
    sums = [sums[0]] + xor_all(sums[1:], "ep", ep_count)
    rows_scratch = ((seq_count, 2 * heads, LANES), F32)
    (normed,) = call(
        attend_kernel,
        "attend",
        [((seq_count, heads * VD), BF16)],
        [lengths, head_lambda]
        + sums
        + [
            cosine,
            sine,
            head_gain[None, :],
            key_cache.reshape(seq_count, cache * kv_local, 2 * SUB),
            value_cache.reshape(seq_count, cache * kv_local, VD),
        ],
        scalars=2,
        scratch=[rows_scratch] * 4,
        cost=OVERLAP,
        ep_count=ep_count,
        group=min(8, seq_count),
    )
    all_heads = [normed] + xor_all([normed] * (ep_count - 1), "ep", ep_count)
    part = (total_rows, slice_width)
    parts = call(
        out_kernel,
        "outproj",
        [(part, F32)] + [(part, BF16)] * (ratio - 1),
        all_heads + [out_weight],
        scratch=[((total_rows, block_width), F32)],
        ep_count=ep_count,
        ratio=ratio,
    )
    parts = [parts[0]] + [
        xor_permute(parts[d], "tp", tp_count, d) for d in range(1, ratio)
    ]
    (part_sum,) = call(add_kernel, "pairsum", [(part, BF16)], parts)

    def device(ep, place, side):
        return ep * tp_count + place * ratio + side

    groups = [(c, h) for c in range(ep_count) for h in range(ratio)]
    both = ("ep", "tp")
    gathered = [part_sum] + [
        lax.ppermute(part_sum, both, [(device(c, c ^ d, h), device(c, c, h)) for c, h in groups])
        for d in range(1, ep_count)
    ]
    (residual,) = call(
        residual_kernel,
        "residual",
        [(part, BF16)],
        gathered + pieces,
        ep_count=ep_count,
        ratio=ratio,
    )
    arrivals = [
        lax.ppermute(residual, both, [(device(c, c, h), device(c ^ d, c, h)) for c, h in groups])
        for d in range(1, ep_count)
    ]

    width = expert_width + dense_width * (total_rows // slot_count)
    place_count = tp_count // 2
    bits = []
    piece_width, piece_rows = width // 2, slot_count
    for _ in range(place_count.bit_length() - 1):
        bits.append(piece_width % (2 * LANES) == 0)
        if bits[-1]:
            piece_width //= 2
        else:
            piece_rows //= 2
    bits = tuple(bits)
    full_rows = slot_count + TAIL
    half = (2, full_rows, width // 2)
    placed, info = call(
        routing_kernel,
        "routing",
        [((slot_count, total_rows), F32), ((total_rows, LANES), F32)],
        pieces,
        ep_count=ep_count,
        local_experts=local_experts,
    )
    sent, kept, own_rows = call(
        experts_kernel,
        "experts",
        [
            (half, BF16),
            (half, F32),
            ((seq_count, slice_width), F32),
        ],
        [residual]
        + arrivals
        + [
            placed,
            first_gain[None, :],
            dense_mix[None, :],
            expert_gate,
            expert_up,
            dense_gate,
            dense_up,
        ],
        scratch=[((2, full_rows, width), F32)],
        mib=8,
        ep_count=ep_count,
        ratio=ratio,
        width=piece_width,
    )
    got = xor_permute(sent, "tp", tp_count, 1)
    piece_tail = -(-(2 * max(1, piece_rows // expert_rows) + STATS) // 8) * 8
    piece = (2 * piece_rows + piece_tail, piece_width)
    parts = call(
        spread_kernel,
        "spread",
        [(piece, F32)] + [(piece, BF16)] * (place_count - 1),
        [kept, got],
        scratch=[(half, F32), ((piece_tail, piece_width), F32)],
        bits=bits,
        expert_rows=expert_rows,
        total_rows=total_rows,
    )
    parts = [parts[0]] + places_all(parts[1:], tp_count)
    act, stats = call(
        act_kernel,
        "act",
        [((1, piece_rows, piece_width), BF16), ((8, total_rows), F32)],
        parts + [placed],
        model_width=model_width,
        expert_width=expert_width,
        dense_width=dense_width,
        expert_rows=expert_rows,
        bits=bits,
    )
    act = jnp.concatenate([act] + places_all([act] * (place_count - 1), tp_count), axis=0)
    act = jnp.concatenate([act, xor_permute(act, "tp", tp_count, 1)], axis=0)
    places = []
    for index in range(tp_count):
        row, column = piece_at(index % place_count, bits, slot_count, width // 2)
        places.append((row, column + index // place_count * (width // 2)))
    mixed = call(
        down_kernel,
        "down",
        [((seq_count, slice_width), F32)]
        + [((seq_count, slice_width), BF16)] * (ep_count - 1),
        [act, stats, info, own_rows, first_gain[None, :], expert_down, dense_down],
        scratch=[((slot_count, width), BF16)],
        ep_count=ep_count,
        places=tuple(places),
    )
    mixed = [mixed[0]] + xor_all(mixed[1:], "ep", ep_count)
    combined, moments = call(
        combine_kernel,
        "combine",
        [((seq_count, slice_width), F32), ((8, LANES), F32)],
        mixed,
    )
    moments = moments + xor_permute(moments, "tp", tp_count, 1)
    others = places_all([moments] * (place_count - 1), tp_count)
    (layer_out,) = call(
        norm_kernel,
        "norm",
        [((seq_count, slice_width), BF16)],
        [combined, second_gain[None, :], moments] + others,
        model_width=model_width,
    )
    return layer_out


def solution(mesh):
    return jax.shard_map(
        on_device,
        mesh=mesh,
        in_specs=(
            P("ep", None),
            P("ep", "tp"),
            P("ep", "tp"),
            P("ep", "tp"),
            P("tp", "ep"),
            P("tp"),
            P(),
            P("ep", None, "tp", None),
            P("ep", None, "tp", None),
            P("ep"),
            P(),
            P("tp"),
            P("ep", None),
            P("ep", None),
            P("ep", "tp", None),
            P("ep", "tp", None),
            P("ep", None, "tp"),
            P("tp", "ep"),
            P("tp", "ep"),
            P("ep", "tp"),
            P(),
        ),
        out_specs=P("ep", "tp"),
        check_vma=False,
    )
```

```python
import functools
import math

import jax
import jax.numpy as jnp
from jax import lax
from jax.experimental import pallas as pl
from jax.experimental.pallas import tpu as pltpu
from jax.sharding import PartitionSpec as P

SUB = 64
VD = 128
TOPK = 2
CAP = 4
LANES = 128
TAIL = 8
STATS = 4

theta_base = 500000.0
score_scale = 0.125
head_scale = 0.8
residual_scale = 2.0**0.5
layer_epsilon = 1e-05
head_epsilon = 1e-06

F32 = jnp.float32
BF16 = jnp.bfloat16

OVERLAP = 20_000_000_000

IN_VMEM = pl.BlockSpec(memory_space=pltpu.VMEM)
IN_SMEM = pl.BlockSpec(memory_space=pltpu.SMEM)


def call(kernel, name, outs, args, scalars=0, scratch=(), mib=4, cost=0, **sizes):
    return pl.pallas_call(
        functools.partial(kernel, **sizes),
        out_shape=[jax.ShapeDtypeStruct(shape, dtype) for shape, dtype in outs],
        in_specs=[IN_SMEM] * scalars + [IN_VMEM] * (len(args) - scalars),
        out_specs=[IN_VMEM] * len(outs),
        scratch_shapes=[pltpu.VMEM(shape, dtype) for shape, dtype in scratch],
        compiler_params=pltpu.CompilerParams(vmem_limit_bytes=mib * 1024 * 1024),
        cost_estimate=pl.CostEstimate(flops=cost, bytes_accessed=cost, transcendentals=0) if cost else None,
        name=name,
    )(*args)


def xor_permute(array, axis, count, distance):
    return lax.ppermute(array, axis, [(i, i ^ distance) for i in range(count)])


def xor_all(arrays, axis, count):
    return [xor_permute(arrays[d - 1], axis, count, d) for d in range(1, count)]


def places_all(arrays, tp_count):
    got = {}
    order = sorted(range(1, tp_count // 2), key=lambda d: (d != 1, -d))
    for d in order:
        got[d] = xor_permute(arrays[d - 1], "tp", tp_count, 2 * d)
    return [got[d] for d in range(1, tp_count // 2)]


def aligned(index, size):
    return pl.ds(pl.multiple_of(index * size, LANES), size)


def iota(shape, dim):
    return lax.broadcasted_iota(jnp.int32, shape, dim)


def row_of(column):
    size = column.shape[0]
    eye = iota((size, size), 0) == iota((size, size), 1)
    return jnp.sum(jnp.where(eye, column, 0.0), axis=0, keepdims=True)


def column_of(row, start, size):
    width = row.shape[1]
    eye = iota((size, width), 0) + start == iota((size, width), 1)
    return jnp.sum(jnp.where(eye, row, 0.0), axis=1, keepdims=True)


def pieces_of(value, count):
    parts = []
    for _ in range(count):
        part = value.astype(BF16).astype(F32)
        parts.append(part)
        value = value - part
    return parts


WEIGHT_LANE = TOPK
MEAN_LANE = WEIGHT_LANE + 3 * TOPK


def prepare_kernel(tokens, ids, weights, *outs, ep_count):
    seq_count, width = tokens.shape
    block = width // ep_count
    ep = lax.axis_index("ep")
    lane = iota((seq_count, LANES), 1)
    extra = jnp.zeros((seq_count, LANES), F32)
    fields = []
    for k in range(TOPK):
        fields.append((k, column_of(ids[k : k + 1, :].astype(F32), 0, seq_count)))
        weight = column_of(weights[k : k + 1, :], 0, seq_count)
        for i, part in enumerate(pieces_of(weight, 3)):
            fields.append((WEIGHT_LANE + 3 * k + i, part))
    mean = jnp.sum(tokens[...].astype(F32), axis=1, keepdims=True) * (1.0 / width)
    for i, part in enumerate(pieces_of(mean, 3)):
        fields.append((MEAN_LANE + i, part))
    for place, value in fields:
        extra = jnp.where(lane == place, value, extra)
    extra = extra.astype(BF16)
    for d in range(ep_count):
        outs[d][:, :block] = tokens[:, aligned(ep ^ d, block)]
        outs[d][:, block:] = extra


def tables_kernel(lengths, cos_ref, sin_ref):
    seq_count = cos_ref.shape[0]
    lane = iota((seq_count, LANES), 1)
    row = iota((seq_count, LANES), 0)
    position = jnp.zeros((seq_count, LANES), F32)
    for s in range(seq_count):
        position = jnp.where(row == s, lengths[s].astype(F32), position)
    rate = (lane % (SUB // 2)).astype(F32) * (-2.0 / SUB * math.log(theta_base))
    angle = position * jnp.exp(rate)
    low_half = (lane % SUB) < (SUB // 2)
    sine = jnp.sin(angle)
    cos_ref[...] = jnp.cos(angle)
    sin_ref[...] = jnp.where(low_half, -sine, sine)


def project_kernel(*refs, ep_count):
    pieces, weights, outs = refs[:ep_count], refs[ep_count : ep_count + 3], refs[ep_count + 3 :]
    rows = pieces[0].shape[0]
    block = weights[0].shape[0]
    columns = jnp.concatenate([piece[:, :block] for piece in pieces], axis=0)
    start = 0
    for weight in weights:
        size = weight.shape[1]
        part = jnp.dot(columns, weight[...], preferred_element_type=F32)
        for d in range(ep_count):
            outs[d][:, start : start + size] = part[d * rows : (d + 1) * rows].astype(
                outs[d].dtype
            )
        start += size


def attend_kernel(lengths, lambdas, *refs, ep_count, group):
    sums = refs[:ep_count]
    cos_ref, sin_ref, gain, keys, values, out, query_rows, key_rows, value_rows, out_rows = refs[
        ep_count:
    ]
    seq_count = keys.shape[0]
    heads = lambdas.shape[0]
    kv_local = (sums[0].shape[1] // LANES - heads) // 2
    per_kv = heads // kv_local
    width = keys.shape[1]
    rows = 2 * heads
    cosine = cos_ref[...]
    sine = sin_ref[...]
    lane = iota((seq_count, LANES), 1)
    low_half = (lane % SUB) < (SUB // 2)
    first_sub = lane < SUB

    def column(index):
        place = slice(index * LANES, (index + 1) * LANES)
        total = sums[0][:, place]
        for other in sums[1:]:
            total = total + other[:, place].astype(F32)
        return total.astype(BF16).astype(F32)

    def rotated(block):
        swapped = jnp.where(
            low_half, pltpu.roll(block, LANES - SUB // 2, 1), pltpu.roll(block, SUB // 2, 1)
        )
        return (block * cosine + swapped * sine).astype(BF16).astype(F32)

    for h in range(heads):
        turned = rotated(column(h)) * score_scale
        query_rows[:, h, :] = jnp.where(first_sub, turned, 0.0)
        query_rows[:, heads + h, :] = jnp.where(first_sub, 0.0, turned)
    for k in range(kv_local):
        turned = rotated(column(heads + k))
        fresh_value = column(heads + kv_local + k)
        for g in range(per_kv):
            for place in (k * per_kv + g, heads + k * per_kv + g):
                key_rows[:, place, :] = turned
                value_rows[:, place, :] = fresh_value

    row_kv = (iota((rows, width), 0) % heads) // per_kv
    place = iota((rows, width), 1)
    position = jnp.where((place % kv_local) == row_kv, place // kv_local, width)
    head_row = iota((rows, 1), 0)
    head_weight = jnp.ones((rows, 1), F32)
    for h in range(heads):
        head_weight = jnp.where(head_row == heads + h, -lambdas[h], head_weight)

    def several(step, carry):
        base = step * group
        scores, mixed = [], []
        for u in range(group):
            part = lax.dot_general(
                query_rows[base + u].astype(BF16),
                keys[base + u],
                (((1,), (1,)), ((), ())),
                preferred_element_type=F32,
            )
            scores.append(jnp.where(position < lengths[base + u], part, -jnp.inf))
        for u in range(group):
            fresh = jnp.sum(
                query_rows[base + u] * key_rows[base + u], axis=1, keepdims=True
            )
            highest = jnp.maximum(jnp.max(scores[u], axis=1, keepdims=True), fresh)
            weight = jnp.exp(scores[u] - highest)
            fresh_weight = jnp.exp(fresh - highest)
            factor = head_weight / (jnp.sum(weight, axis=1, keepdims=True) + fresh_weight)
            weight = weight * factor
            fresh_weight = jnp.broadcast_to(fresh_weight * factor, (rows, LANES))
            mixed.append((weight + pltpu.roll(weight, heads, 0)).astype(BF16))
            fresh_weight = fresh_weight + pltpu.roll(fresh_weight, heads, 0)
            out_rows[base + u] = fresh_weight.astype(BF16).astype(F32) * value_rows[base + u]
        for u in range(group):
            out_rows[base + u] += jnp.dot(
                mixed[u], values[base + u], preferred_element_type=F32
            )
        return carry

    lax.fori_loop(0, seq_count // group, several, 0)
    for h in range(heads):
        head = out_rows[:, h, :]
        square_mean = jnp.mean(head * head, axis=1, keepdims=True)
        normed = head * lax.rsqrt(square_mean + head_epsilon) * gain[...] * head_scale
        out[:, h * LANES : (h + 1) * LANES] = normed.astype(BF16)


def out_kernel(*refs, ep_count, ratio):
    heads, weight, outs, full = (
        refs[:ep_count],
        refs[ep_count],
        refs[ep_count + 1 : ep_count + 1 + ratio],
        refs[-1],
    )
    rows = jnp.concatenate([ref[...] for ref in heads], axis=0)
    full[...] = jnp.dot(rows, weight[...], preferred_element_type=F32)
    side = lax.axis_index("tp") % ratio
    size = outs[0].shape[1]
    for d in range(ratio):
        outs[d][...] = full[:, aligned(side ^ d, size)].astype(outs[d].dtype)


def add_kernel(*refs):
    total = refs[0][...].astype(F32)
    for ref in refs[1:-1]:
        total = total + ref[...].astype(F32)
    refs[-1][...] = total.astype(refs[-1].dtype)


def residual_kernel(*refs, ep_count, ratio):
    sums, pieces, out = refs[:ep_count], refs[ep_count : 2 * ep_count], refs[-1]
    rows = pieces[0].shape[0]
    size = out.shape[1]
    side = lax.axis_index("tp") % ratio
    block = pieces[0].shape[1] - LANES
    for d in range(ep_count):
        place = slice(d * rows, (d + 1) * rows)
        total = sums[0][place, :].astype(F32)
        for other in sums[1:]:
            total = total + other[place, :].astype(F32)
        extra = pieces[d][:, block:].astype(F32)
        mean = extra[:, MEAN_LANE : MEAN_LANE + 1]
        for i in range(1, 3):
            mean = mean + extra[:, MEAN_LANE + i : MEAN_LANE + i + 1]
        own = pieces[d][:, aligned(side, size)].astype(F32)
        out[place, :] = (residual_scale * (own - mean) + total).astype(BF16)


def routing_kernel(*refs, ep_count, local_experts):
    pieces, placed_out, info_out = refs[:ep_count], refs[-2], refs[-1]
    ep = lax.axis_index("ep")
    seq_count = pieces[0].shape[0]
    slot_count, total_rows = placed_out.shape
    expert_rows = ep_count * CAP

    block = pieces[0].shape[1] - LANES
    extra = jnp.concatenate([piece[:, block:] for piece in pieces], axis=0).astype(F32)
    token_row = iota((total_rows, total_rows), 0)
    token_lane = iota((total_rows, total_rows), 1)
    earlier = (token_lane < token_row) & (token_lane // seq_count == token_row // seq_count)
    ids = [extra[:, k : k + 1] for k in range(TOPK)]
    id_rows = [row_of(column) for column in ids]
    weights = []
    for k in range(TOPK):
        first = WEIGHT_LANE + 3 * k
        weights.append(
            extra[:, first : first + 1]
            + extra[:, first + 1 : first + 2]
            + extra[:, first + 2 : first + 3]
        )
    weight_sum = weights[0]
    for k in range(1, TOPK):
        weight_sum = weight_sum + weights[k]
    token_block = (iota((total_rows, 1), 0) // seq_count).astype(F32)
    slot_row = iota((slot_count, total_rows), 0).astype(F32)
    placed = jnp.zeros((slot_count, total_rows), F32)
    info = jnp.zeros((total_rows, LANES), F32)
    info_lane = iota((total_rows, LANES), 1)
    first_expert = (ep * local_experts).astype(F32)
    for k in range(TOPK):
        same = jnp.zeros((total_rows, total_rows), F32)
        for other in id_rows:
            same = same + jnp.where(earlier & (ids[k] == other), 1.0, 0.0)
        rank = jnp.sum(same, axis=1, keepdims=True)
        local = ids[k] - first_expert
        slot = local * expert_rows + token_block * CAP + rank
        slot = jnp.where((local >= 0.0) & (local < local_experts), slot, -1.0)
        placed = placed + jnp.where(slot_row == row_of(slot), 1.0, 0.0)
        info = jnp.where(info_lane == k, slot, info)
        info = jnp.where(info_lane == TOPK + k, weights[k] / weight_sum, info)
    info_out[...] = info
    placed_out[...] = placed


def experts_kernel(*refs, ep_count, ratio, width, plane):
    own = refs[0]
    arrivals = refs[1:ep_count]
    (
        placed,
        gain_ref,
        mix_ref,
        expert_weight_ref,
        dense_weight,
        sent,
        kept,
        *own_out,
        full,
    ) = refs[ep_count:]
    ep = lax.axis_index("ep")
    tp = lax.axis_index("tp")
    total_rows, size = own.shape
    seq_count = total_rows // ep_count
    local_experts = expert_weight_ref.shape[0]
    expert_rows = ep_count * CAP
    slot_count = local_experts * expert_rows
    distance = ep ^ (tp // ratio)
    blocks = []
    for i in range(ep_count):
        rows = own[i * seq_count : (i + 1) * seq_count, :].astype(F32)
        rows = jnp.where(distance == 0, rows, 0.0)
        for d in range(1, ep_count):
            j = i ^ d
            rows = rows + arrivals[d - 1][j * seq_count : (j + 1) * seq_count, :].astype(F32)
        blocks.append(rows)
    if own_out:
        own_out[0][...] = blocks[0]
    rows = jnp.concatenate(blocks, axis=0)
    gain = gain_ref[:, aligned(tp, size)]
    mix = mix_ref[:, aligned(tp, size)].astype(F32)
    scaled = rows * gain
    hidden = scaled.astype(BF16)

    routed = jnp.dot(placed[...].astype(BF16), hidden, preferred_element_type=F32).astype(BF16)

    sums = [
        jnp.sum(rows, axis=1, keepdims=True),
        jnp.sum(rows * rows, axis=1, keepdims=True),
        jnp.sum(scaled * mix, axis=1, keepdims=True),
        jnp.broadcast_to(jnp.sum(gain * mix, axis=1, keepdims=True), (total_rows, 1)),
    ]
    gain_high = gain.astype(BF16).astype(F32)
    gain_row = iota((16, size), 0)
    gain_rows = jnp.where(
        gain_row == 0, gain_high, jnp.where(gain_row == 1, gain - gain_high, 0.0)
    ).astype(BF16)
    expert_width = expert_weight_ref.shape[2]
    dense_width = dense_weight.shape[1]
    fold = total_rows // slot_count
    full[slot_count:, :] = jnp.zeros((TAIL, full.shape[1]), F32)
    dense_rows = jnp.concatenate([hidden, gain_rows], axis=0)
    for e in range(local_experts):
        lhs = jnp.concatenate(
            [routed[e * expert_rows : (e + 1) * expert_rows], gain_rows], axis=0
        )
        part = jnp.dot(lhs, expert_weight_ref[e], preferred_element_type=F32)
        full[e * expert_rows : (e + 1) * expert_rows, :expert_width] = part[
            :expert_rows
        ]
        full[slot_count + e : slot_count + e + 1, :expert_width] = (
            part[expert_rows : expert_rows + 1] + part[expert_rows + 1 : expert_rows + 2]
        )
    part = jnp.dot(dense_rows, dense_weight[...], preferred_element_type=F32)
    gain_part = part[total_rows : total_rows + 1] + part[total_rows + 1 : total_rows + 2]
    for f in range(fold):
        place = slice(expert_width + f * dense_width, expert_width + (f + 1) * dense_width)
        full[:slot_count, place] = part[f * slot_count : (f + 1) * slot_count]
        for e in range(local_experts):
            full[slot_count + e : slot_count + e + 1, place] = gain_part
    half = full.shape[1] // 2
    side = tp & 1
    sent[...] = full[:, aligned(1 - side, half)].astype(BF16)
    kept[...] = full[:, aligned(side, half)]
    sums = jnp.concatenate([row_of(column) for column in sums], axis=0)
    high = sums.astype(BF16)
    rows = slice(slot_count + TAIL - STATS, slot_count + TAIL)
    for start in range(0, half, width):
        place = slice(start, start + total_rows)
        if plane == 0:
            sent[rows, place] = high
            kept[rows, place] = sums
        else:
            sent[rows, place] = (sums - high.astype(F32)).astype(BF16)


def piece_at(index, bits, rows, width):
    row, column = 0, 0
    for bit, splits_columns in enumerate(bits):
        up = (index >> bit) & 1
        if splits_columns:
            width //= 2
            column = column + up * width
        else:
            rows //= 2
            row = row + up * rows
    return row, column


def low_lane(total_rows):
    return -(-total_rows // LANES) * LANES


def spread_kernel(*refs, bits, expert_rows, total_rows):
    outs, full, tail = refs[4:-2], refs[-2], refs[-1]
    for plane in range(2):
        full[plane] = refs[plane][...] + refs[2 + plane][...].astype(F32)
    slot_count = full.shape[1] - TAIL
    width = outs[0].shape[1]
    piece_rows = (outs[0].shape[0] - tail.shape[0]) // 2
    experts = max(1, piece_rows // expert_rows)
    place = lax.axis_index("tp") >> 1
    low = low_lane(total_rows)
    for d, out in enumerate(outs):
        row, column = piece_at(place ^ d, bits, slot_count, full.shape[2])
        lanes = pl.ds(pl.multiple_of(column, LANES), width)
        first = slot_count + row // expert_rows
        tail[...] = jnp.zeros(tail.shape, F32)
        for plane in range(2):
            main = full[plane, pl.ds(pl.multiple_of(row, 8), piece_rows), lanes]
            out[plane * piece_rows : (plane + 1) * piece_rows, :] = main.astype(out.dtype)
            for i in range(experts):
                at = plane * experts + i
                tail[at : at + 1, :] = full[plane, pl.ds(first + i, 1), lanes]
        sums = full[:, slot_count + TAIL - STATS :, lanes]
        sums = (sums[0] + sums[1])[:, :total_rows]
        rows = slice(2 * experts, 2 * experts + STATS)
        if d:
            high = sums.astype(BF16).astype(F32)
            tail[rows, :total_rows] = high
            tail[rows, low : low + total_rows] = sums - high
        else:
            tail[rows, :total_rows] = sums
        out[2 * piece_rows :, :] = tail[...].astype(out.dtype)


def act_kernel(
    *refs, model_width, expert_width, dense_width, expert_rows, bits
):
    placed, act, stats = refs[-3:]
    total = refs[0][...]
    for ref in refs[1:-3]:
        total = total + ref[...].astype(F32)
    rows, width = act.shape[1:]
    slot_count, total_rows = placed.shape
    experts = max(1, rows // expert_rows)
    tp = lax.axis_index("tp")
    low = low_lane(total_rows)
    sums = total[2 * (rows + experts) : 2 * (rows + experts) + STATS, :]
    sums = sums[:, :total_rows] + sums[:, low : low + total_rows]
    mean = sums[0:1] * (1.0 / model_width)
    variance = sums[1:2] * (1.0 / model_width) - mean * mean
    scale = lax.rsqrt(variance + layer_epsilon)
    gate = jax.nn.sigmoid(scale * (sums[2:3] - mean * sums[3:4]))
    stats[0:1, :] = mean
    stats[1:2, :] = scale
    stats[2:3, :] = gate
    whole = expert_width + dense_width * (total_rows // slot_count)
    first_row, first_column = piece_at(tp >> 1, bits, slot_count, whole // 2)
    first_column = first_column + (tp & 1) * (whole // 2)
    mine = placed[pl.ds(pl.multiple_of(first_row, 8), rows), :]
    scale_used = jnp.sum(mine * scale, axis=1, keepdims=True)
    mean_used = jnp.sum(mine * mean, axis=1, keepdims=True)
    column = iota((rows, width), 1) + first_column
    scale_used = jnp.broadcast_to(scale_used, (rows, width))
    mean_used = jnp.broadcast_to(mean_used, (rows, width))
    for f in range(total_rows // slot_count):
        dense = column >= expert_width + f * dense_width
        start = first_row + f * slot_count
        scale_used = jnp.where(dense, column_of(scale, start, rows), scale_used)
        mean_used = jnp.where(dense, column_of(mean, start, rows), mean_used)
    expert = iota((rows, width), 0) // expert_rows
    pre = []
    for plane in range(2):
        gain_sum = jnp.zeros((rows, width), F32)
        for i in range(experts):
            at = 2 * rows + plane * experts + i
            gain_sum = jnp.where(expert == i, total[at : at + 1, :], gain_sum)
        main = total[plane * rows : (plane + 1) * rows, :]
        pre.append(scale_used * (main - mean_used * gain_sum))
    act[0] = (pre[0] / (1.0 + jnp.exp(-pre[0])) * pre[1]).astype(BF16)


def down_kernel(
    acts,
    stats,
    info,
    own_rows,
    gain_ref,
    expert_down,
    dense_down,
    *refs,
    ep_count,
    places,
):
    outs, joined = refs[:ep_count], refs[ep_count]
    tp = lax.axis_index("tp")
    piece_rows, piece_width = acts.shape[1:]
    for index, (row, column) in enumerate(places):
        block = acts[index ^ ((tp & 1) * (len(places) // 2) + (tp >> 1))]
        joined[row : row + piece_rows, column : column + piece_width] = block
    local_experts, expert_width, size = expert_down.shape
    dense_width = dense_down.shape[0]
    slot_count = joined.shape[0]
    expert_rows = slot_count // local_experts
    total_rows = info.shape[0]
    seq_count = total_rows // ep_count
    results = []
    for e in range(local_experts):
        lhs = joined[e * expert_rows : (e + 1) * expert_rows, :expert_width]
        results.append(jnp.dot(lhs, expert_down[e], preferred_element_type=F32))
    result = jnp.concatenate(results, axis=0).astype(BF16)
    fold = total_rows // slot_count
    dense_rows = jnp.concatenate(
        [
            joined[:, expert_width + f * dense_width : expert_width + (f + 1) * dense_width]
            for f in range(fold)
        ],
        axis=0,
    )
    dense = jnp.dot(dense_rows, dense_down[...], preferred_element_type=F32)
    mixed = column_of(stats[2:3, :], 0, total_rows) * dense
    slot_lane = iota((total_rows, slot_count), 1).astype(F32)
    for k in range(TOPK):
        chosen = jnp.where(info[:, k : k + 1] == slot_lane, 1.0, 0.0).astype(BF16)
        picked = jnp.dot(chosen, result, preferred_element_type=F32)
        mixed = mixed + info[:, TOPK + k : TOPK + k + 1] * picked
    gain = gain_ref[:, aligned(tp, size)]
    mean = column_of(stats[0:1, :], 0, seq_count)
    scale = column_of(stats[1:2, :], 0, seq_count)
    hidden = (own_rows[...] - mean) * scale * gain
    outs[0][...] = mixed[:seq_count] + residual_scale * hidden
    for d in range(1, ep_count):
        outs[d][...] = mixed[d * seq_count : (d + 1) * seq_count].astype(BF16)


def combine_kernel(*refs):
    combined, moments = refs[-2:]
    total = refs[0][...]
    for ref in refs[1:-2]:
        total = total + ref[...].astype(F32)
    combined[...] = total
    moments[...] = jnp.zeros(moments.shape, F32)
    rows = total.shape[0]
    moments[0:1, :rows] = row_of(jnp.sum(total, axis=1, keepdims=True))
    moments[1:2, :rows] = row_of(jnp.sum(total * total, axis=1, keepdims=True))


def norm_kernel(*refs, model_width):
    combined, gain = refs[0], refs[1]
    out = refs[-1]
    sums = refs[2][...]
    for ref in refs[3:-1]:
        sums = sums + ref[...]
    mean = sums[0:1] * (1.0 / model_width)
    variance = sums[1:2] * (1.0 / model_width) - mean * mean
    rows = combined.shape[0]
    scale = column_of(lax.rsqrt(variance + layer_epsilon), 0, rows)
    out[...] = ((combined[...] - column_of(mean, 0, rows)) * scale * gain[...]).astype(BF16)


def on_device(
    tokens,
    query_weight,
    key_weight,
    value_weight,
    out_weight,
    head_lambda,
    head_gain,
    key_cache,
    value_cache,
    lengths,
    first_gain,
    second_gain,
    expert_ids,
    route_weights,
    expert_gate,
    expert_up,
    expert_down,
    dense_gate,
    dense_up,
    dense_down,
    dense_mix,
):
    seq_count, model_width = tokens.shape
    ep_count = lax.axis_size("ep")
    tp_count = lax.axis_size("tp")
    ratio = tp_count // ep_count
    block_width = model_width // ep_count
    slice_width = model_width // tp_count
    local_experts, _, expert_width = expert_gate.shape
    dense_width = dense_gate.shape[1]
    expert_rows = ep_count * CAP
    slot_count = local_experts * expert_rows
    total_rows = ep_count * seq_count
    heads = head_lambda.shape[0]
    cache, kv_local = key_cache.shape[1:3]

    piece = ((seq_count, block_width + LANES), BF16)
    table = ((seq_count, LANES), F32)
    pieces = call(
        prepare_kernel,
        "prepare",
        [piece] * ep_count,
        [
            pltpu.with_memory_space_constraint(array, pltpu.HBM)
            for array in (tokens, expert_ids.T, route_weights.T)
        ],
        cost=OVERLAP,
        ep_count=ep_count,
    )
    cosine, sine = call(tables_kernel, "tables", [table] * 2, [lengths], scalars=1)
    pieces = [pieces[0]] + xor_all(pieces[1:], "ep", ep_count)
    qkv_width = (heads + 2 * kv_local) * LANES
    sums = call(
        project_kernel,
        "project",
        [((seq_count, qkv_width), F32)] + [((seq_count, qkv_width), BF16)] * (ep_count - 1),
        pieces + [query_weight, key_weight, value_weight],
        ep_count=ep_count,
    )
    sums = [sums[0]] + xor_all(sums[1:], "ep", ep_count)
    rows_scratch = ((seq_count, 2 * heads, LANES), F32)
    (normed,) = call(
        attend_kernel,
        "attend",
        [((seq_count, heads * VD), BF16)],
        [lengths, head_lambda]
        + sums
        + [
            cosine,
            sine,
            head_gain[None, :],
            key_cache.reshape(seq_count, cache * kv_local, 2 * SUB),
            value_cache.reshape(seq_count, cache * kv_local, VD),
        ],
        scalars=2,
        scratch=[rows_scratch] * 4,
        cost=OVERLAP,
        ep_count=ep_count,
        group=min(8, seq_count),
    )
    all_heads = [normed] + xor_all([normed] * (ep_count - 1), "ep", ep_count)
    part = (total_rows, slice_width)
    parts = call(
        out_kernel,
        "outproj",
        [(part, F32)] + [(part, BF16)] * (ratio - 1),
        all_heads + [out_weight],
        scratch=[((total_rows, block_width), F32)],
        ep_count=ep_count,
        ratio=ratio,
    )
    parts = [parts[0]] + [
        xor_permute(parts[d], "tp", tp_count, d) for d in range(1, ratio)
    ]
    (part_sum,) = call(add_kernel, "pairsum", [(part, BF16)], parts)

    def device(ep, place, side):
        return ep * tp_count + place * ratio + side

    groups = [(c, h) for c in range(ep_count) for h in range(ratio)]
    both = ("ep", "tp")
    gathered = [part_sum] + [
        lax.ppermute(part_sum, both, [(device(c, c ^ d, h), device(c, c, h)) for c, h in groups])
        for d in range(1, ep_count)
    ]
    (residual,) = call(
        residual_kernel,
        "residual",
        [(part, BF16)],
        gathered + pieces,
        ep_count=ep_count,
        ratio=ratio,
    )
    arrivals = [
        lax.ppermute(residual, both, [(device(c, c, h), device(c ^ d, c, h)) for c, h in groups])
        for d in range(1, ep_count)
    ]

    width = expert_width + dense_width * (total_rows // slot_count)
    place_count = tp_count // 2
    bits = []
    piece_width, piece_rows = width // 2, slot_count
    for _ in range(place_count.bit_length() - 1):
        bits.append(piece_width % (2 * LANES) == 0)
        if bits[-1]:
            piece_width //= 2
        else:
            piece_rows //= 2
    bits = tuple(bits)
    full_rows = slot_count + TAIL
    half = (full_rows, width // 2)
    placed, info = call(
        routing_kernel,
        "routing",
        [((slot_count, total_rows), F32), ((total_rows, LANES), F32)],
        pieces,
        ep_count=ep_count,
        local_experts=local_experts,
    )
    kept, got = [], []
    for plane, (name, expert_weight, dense_weight) in enumerate(
        (("gates", expert_gate, dense_gate), ("ups", expert_up, dense_up))
    ):
        outs = [(half, BF16), (half, F32)]
        if plane == 0:
            outs.append(((seq_count, slice_width), F32))
        result = call(
            experts_kernel,
            name,
            outs,
            [residual]
            + arrivals
            + [placed, first_gain[None, :], dense_mix[None, :], expert_weight, dense_weight],
            scratch=[((full_rows, width), F32)],
            mib=8,
            ep_count=ep_count,
            ratio=ratio,
            width=piece_width,
            plane=plane,
        )
        if plane == 0:
            own_rows = result[2]
        kept.append(result[1])
        got.append(xor_permute(result[0], "tp", tp_count, 1))
    piece_tail = -(-(2 * max(1, piece_rows // expert_rows) + STATS) // 8) * 8
    piece = (2 * piece_rows + piece_tail, piece_width)
    parts = call(
        spread_kernel,
        "spread",
        [(piece, F32)] + [(piece, BF16)] * (place_count - 1),
        kept + got,
        scratch=[((2,) + half, F32), ((piece_tail, piece_width), F32)],
        bits=bits,
        expert_rows=expert_rows,
        total_rows=total_rows,
    )
    parts = [parts[0]] + places_all(parts[1:], tp_count)
    act, stats = call(
        act_kernel,
        "act",
        [((1, piece_rows, piece_width), BF16), ((8, total_rows), F32)],
        parts + [placed],
        model_width=model_width,
        expert_width=expert_width,
        dense_width=dense_width,
        expert_rows=expert_rows,
        bits=bits,
    )
    act = jnp.concatenate([act] + places_all([act] * (place_count - 1), tp_count), axis=0)
    act = jnp.concatenate([act, xor_permute(act, "tp", tp_count, 1)], axis=0)
    places = []
    for index in range(tp_count):
        row, column = piece_at(index % place_count, bits, slot_count, width // 2)
        places.append((row, column + index // place_count * (width // 2)))
    mixed = call(
        down_kernel,
        "down",
        [((seq_count, slice_width), F32)]
        + [((seq_count, slice_width), BF16)] * (ep_count - 1),
        [act, stats, info, own_rows, first_gain[None, :], expert_down, dense_down],
        scratch=[((slot_count, width), BF16)],
        ep_count=ep_count,
        places=tuple(places),
    )
    mixed = [mixed[0]] + xor_all(mixed[1:], "ep", ep_count)
    combined, moments = call(
        combine_kernel,
        "combine",
        [((seq_count, slice_width), F32), ((8, LANES), F32)],
        mixed,
    )
    moments = moments + xor_permute(moments, "tp", tp_count, 1)
    others = places_all([moments] * (place_count - 1), tp_count)
    (layer_out,) = call(
        norm_kernel,
        "norm",
        [((seq_count, slice_width), BF16)],
        [combined, second_gain[None, :], moments] + others,
        model_width=model_width,
    )
    return layer_out


def solution(mesh):
    return jax.shard_map(
        on_device,
        mesh=mesh,
        in_specs=(
            P("ep", None),
            P("ep", "tp"),
            P("ep", "tp"),
            P("ep", "tp"),
            P("tp", "ep"),
            P("tp"),
            P(),
            P("ep", None, "tp", None),
            P("ep", None, "tp", None),
            P("ep"),
            P(),
            P("tp"),
            P("ep", None),
            P("ep", None),
            P("ep", "tp", None),
            P("ep", "tp", None),
            P("ep", None, "tp"),
            P("tp", "ep"),
            P("tp", "ep"),
            P("ep", "tp"),
            P(),
        ),
        out_specs=P("ep", "tp"),
        check_vma=False,
    )
```
